32 devices in a mesh: grp: 2 (over y), sp: 4 (over z), tp: 4 (over x, core).
Axes of the slice: x: 2, y: 2, z: 4, core: 2. Of those that a mesh axis runs over, the one named last changes fastest.
Arguments:
- inputs: bfloat16 [2048, 2048], P(('grp', 'sp'), 'tp'), parts along dimension 0, may hold values from -20 to 20
- norm_gain: bfloat16 [2048], replicated, may hold values from 0.099609375 to 1.8984375
- w_conv_in: bfloat16 [1024, 2048], P('tp'), may hold values from -0.125 to 0.125
- w_conv_gate: bfloat16 [1024, 2048], P('tp'), may hold values from -0.125 to 0.125
- conv_kernel: bfloat16 [31, 1024], P(None, 'tp'), may hold values from -4.3105272 to 4.3105272
- ln_gain: bfloat16 [1024], P('tp'), may hold values from 0.099609375 to 1.8984375
- w_query: bfloat16 [1024, 2048], P('tp'), may hold values from -0.53033009 to 0.53033009
- w_key: bfloat16 [1024, 2048], P('tp'), may hold values from -0.53033009 to 0.53033009
- w_value: bfloat16 [1024, 2048], P('tp'), may hold values from -0.125 to 0.125
- cum_gate: float32 [16, 2048], P('tp', ('grp', 'sp')), parts along dimension 1, may hold values from -1024 to 0, as said below
- w_conv_out: bfloat16 [1024, 2048], P('tp'), may hold values from -0.125 to 0.125
- w_attn_out: bfloat16 [1024, 2048], P('tp'), may hold values from -0.125 to 0.125
Outputs:
- mixed: bfloat16 [2048, 2048], P(('grp', 'sp', 'tp')), parts along dimension 0
- log_total: float32 [16, 2048], P('tp', ('grp', 'sp')), parts along dimension 1
The draws below stay inside these ranges and needn't reach their ends.
There are 2 independent parts, one for each index of `grp`. The reference program is written for one: setup_inputs(seed, part) draws one part's arguments, and reference() takes and returns one part's arrays. A program takes and returns all parts, laid end to end along the dimension named above; an argument that names none is the same for every part. Nothing has to cross between parts.
Inputs may be any that keep to these rules, and one draw needn't show every extreme that they name: cum_gate never rises along positions: entry t is the sum of the head's log forget gates at positions 0 to t.
All inputs are finite; a program needn't handle non-finite values.
Results may differ from the reference program's by a relative error of at most 0.0144.
Values may be sent and summed in bfloat16 or wider, within the bound.
A program may use at most 64 MiB of HBM per device.

```python
import math
import jax
import jax.numpy as jnp
from jax import lax

D = 2048
CONV_CH = 1024
ATTENDER_TOTAL = 16
HEAD_DIM = 64
CONV_WIDTH = 31
TOK_DEV = 256
ATT_W = 1024
SEQUENCE_SPAN = 1024
N_SP = 4
N_TP = 4


def draw_inputs(key, part):
    key_one = jax.random.fold_in(key, 0)
    columns = jnp.exp(jnp.linspace(math.log(0.5), math.log(3.0), D)).astype(jnp.float32)
    raw_draw = jnp.clip(jax.random.normal(key_one, (SEQUENCE_SPAN, D), jnp.float32), -6.0, 6.0)
    return (raw_draw * columns[None, :]).astype(jnp.bfloat16)


def query_key_pair(key):
    query_draw = jnp.clip(jax.random.normal(jax.random.fold_in(key, 11), (ATT_W, D), jnp.float32), -6.0, 6.0) * D ** (-0.5)
    key_draw = 2.0 * jnp.clip(jax.random.normal(jax.random.fold_in(key, 13), (ATT_W, D), jnp.float32), -6.0, 6.0) * D ** (-0.5)
    query_draw = 2.0 * query_draw
    return (query_draw, key_draw)


def draw_w_query(key, part):
    return query_key_pair(key)[0].astype(jnp.bfloat16)


def draw_w_key(key, part):
    return query_key_pair(key)[1].astype(jnp.bfloat16)


def draw_conv_kernel(key, part):
    channels = jnp.exp(jnp.linspace(math.log(0.4), math.log(4.0), CONV_CH)).astype(jnp.float32)
    raw_draw = jnp.clip(jax.random.normal(key, (CONV_WIDTH, CONV_CH), jnp.float32), -6.0, 6.0)
    return (raw_draw * CONV_WIDTH ** (-0.5) * channels[None, :]).astype(jnp.bfloat16)


def draw_cum_gate(key, part):
    derived_seeds = jax.random.split(key, 6)
    head_order = jax.random.permutation(derived_seeds[0], ATTENDER_TOTAL)
    longest_memory_channel = head_order < ATTENDER_TOTAL // 2
    head_rate = jnp.exp(jax.random.uniform(derived_seeds[1], (ATTENDER_TOTAL,), jnp.float32, math.log(0.8), math.log(1.25)))
    base_rate = jnp.where(longest_memory_channel, 0.5 / SEQUENCE_SPAN, 1.0 / 25.0) * head_rate
    block_rate = jnp.exp(jax.random.uniform(derived_seeds[2], (ATTENDER_TOTAL, SEQUENCE_SPAN // TOK_DEV), jnp.float32, math.log(0.5), math.log(2.0)))
    block_rate = jnp.repeat(block_rate, TOK_DEV, axis=1)
    position_rate = jax.random.uniform(derived_seeds[3], (ATTENDER_TOTAL, SEQUENCE_SPAN), jnp.float32, 0.5, 1.5)
    decay_exponent = -base_rate[:, None] * block_rate * position_rate
    contiguous_offset = jax.random.randint(derived_seeds[4], (ATTENDER_TOTAL, 2, 1), 0, SEQUENCE_SPAN)
    contiguous_extent = jax.random.uniform(derived_seeds[5], (ATTENDER_TOTAL, 2, 1), jnp.float32, 0.22, 0.69)
    location_numbers = jnp.arange(SEQUENCE_SPAN, dtype=jnp.int32)
    contiguous_batches = jnp.sum(jnp.where(location_numbers[None, None, :] == contiguous_offset, contiguous_extent, 0.0), axis=1)
    decay_exponent = decay_exponent - jnp.where(longest_memory_channel[:, None], contiguous_batches, 0.0)
    return jnp.cumsum(decay_exponent, axis=1)


def levels(own_key, shape, pieces, least, top_value):
    def one(position, blocks):
        steps = jax.random.uniform(jax.random.fold_in(jax.random.fold_in(own_key, 6), position), (blocks,), jnp.float32, least / len(pieces), top_value / len(pieces))
        return jnp.repeat(jnp.exp(steps), shape[position] // blocks).reshape((-1,) + (1,) * (len(shape) - position - 1))

    level = one(*pieces[0])
    for cut in pieces[1:]:
        level = level * one(*cut)
    return level


def noise(key, shape, spread, most, pieces=(), kind=jnp.bfloat16):
    array = spread * jax.random.normal(key, shape, jnp.float32)
    if pieces:
        array = array * levels(key, shape, pieces, -0.22, 0.18)
    return jnp.clip(array, -most, most).astype(kind)


def setup_inputs(seed: int = 0, part: int = 0) -> dict:
    key_list = jax.random.split(jax.random.key(seed), 13)
    part_splits = jax.random.split(jax.random.fold_in(key_list[12], part), 13)
    return {
        "inputs": draw_inputs(jax.random.fold_in(jax.random.fold_in(key_list[12], part), 71), part),
        "norm_gain": jnp.clip(1.0 + 0.18 * jax.random.normal(key_list[1], (D,), jnp.float32), 0.099609375, 1.8984375).astype(jnp.bfloat16),
        "w_conv_in": noise(key_list[2], (CONV_CH, D), D ** -0.5, 0.125, ((0, 4),)),
        "w_conv_gate": noise(key_list[3], (CONV_CH, D), D ** -0.5, 0.125, ((0, 4),)),
        "conv_kernel": draw_conv_kernel(jax.random.fold_in(key_list[12], 71), part),
        "ln_gain": jnp.clip(1.0 + 0.18 * jax.random.normal(key_list[5], (CONV_CH,), jnp.float32), 0.099609375, 1.8984375).astype(jnp.bfloat16),
        "w_query": draw_w_query(jax.random.fold_in(key_list[12], 71), part),
        "w_key": draw_w_key(jax.random.fold_in(key_list[12], 71), part),
        "w_value": noise(key_list[8], (ATT_W, D), D ** -0.5, 0.125, ((0, 4),)),
        "cum_gate": draw_cum_gate(jax.random.fold_in(jax.random.fold_in(key_list[12], part), 71), part),
        "w_conv_out": noise(key_list[10], (CONV_CH, D), (CONV_CH + ATT_W) ** -0.5, 0.125, ((0, 4),)),
        "w_attn_out": noise(key_list[11], (ATT_W, D), (CONV_CH + ATT_W) ** -0.5, 0.125, ((0, 4),)),
    }


neg_large = -1e+30

def block_terms(q_blk, q_cum, k_blk, v_blk, k_cum, q_first, k_first):
    score_scale = q_blk.shape[2] ** (-0.5)
    scores = jnp.einsum('qhd,khd->hqk', q_blk.astype(jnp.float32), k_blk.astype(jnp.float32)) * score_scale
    scores = scores + q_cum[:, :, None] - k_cum[:, None, :]
    q_pos = q_first + jnp.arange(q_blk.shape[0], dtype=jnp.int32)
    k_pos = k_first + jnp.arange(k_blk.shape[0], dtype=jnp.int32)
    allowed = k_pos[None, :] <= q_pos[:, None]
    scores = jnp.where(allowed[None], scores, -jnp.inf)
    block_top = lax.optimization_barrier(jnp.max(scores, axis=-1))
    weights = jnp.exp(scores - block_top[..., None])
    block_total = lax.optimization_barrier(jnp.sum(weights, axis=-1))
    rounded = lax.optimization_barrier(weights.astype(jnp.bfloat16))
    block_out = jnp.einsum('hqk,khd->hqd', rounded.astype(jnp.float32), v_blk.astype(jnp.float32)).astype(jnp.bfloat16)
    return (block_top, block_total, block_out)

def merge_terms(state, terms):
    top_now, total_now, acc_now = state
    block_top, block_total, block_out = terms
    top_new = jnp.maximum(top_now, block_top)
    keep_old = jnp.exp(top_now - top_new)
    keep_new = jnp.exp(block_top - top_new)
    return (top_new, total_now * keep_old + block_total * keep_new, acc_now * keep_old[..., None] + block_out.astype(jnp.float32) * keep_new[..., None])

def reference(inputs, norm_gain, w_conv_in, w_conv_gate, conv_kernel, ln_gain, w_query, w_key, w_value, cum_gate, w_conv_out, w_attn_out):
    rows_f = inputs.astype(jnp.float32)
    rms = lax.rsqrt(lax.optimization_barrier(jnp.mean(rows_f * rows_f, axis=1, keepdims=True)) + 1e-06)
    scaled = (rows_f * norm_gain.astype(jnp.float32)[None, :]).astype(jnp.bfloat16)

    def project(weight):
        return lax.dot_general(scaled, weight, (((1,), (1,)), ((), ())), preferred_element_type=jnp.float32) * rms
    conv_in = project(w_conv_in)
    conv_gate = project(w_conv_gate)
    glu = (conv_in * jax.nn.sigmoid(conv_gate)).astype(jnp.bfloat16)
    padded = jnp.concatenate([jnp.zeros((CONV_WIDTH - 1, CONV_CH), jnp.bfloat16), glu], axis=0)
    kernel = conv_kernel.astype(jnp.float32)
    conv_sum = jnp.zeros((SEQUENCE_SPAN, CONV_CH), jnp.float32)
    for tap_idx in range(CONV_WIDTH):
        conv_sum = conv_sum + padded[tap_idx:tap_idx + SEQUENCE_SPAN].astype(jnp.float32) * kernel[tap_idx][None, :]
    chan_mean = lax.optimization_barrier(jnp.mean(conv_sum, axis=1, keepdims=True))
    chan_var = lax.optimization_barrier(jnp.mean(conv_sum * conv_sum, axis=1, keepdims=True)) - chan_mean * chan_mean
    normed = (conv_sum - chan_mean) * lax.rsqrt(chan_var + 1e-05) * ln_gain.astype(jnp.float32)[None, :]
    conv_out = jax.nn.silu(normed).astype(jnp.bfloat16)
    query = project(w_query).astype(jnp.bfloat16).reshape(N_SP, TOK_DEV, ATTENDER_TOTAL, HEAD_DIM)
    key_rows = project(w_key).astype(jnp.bfloat16).reshape(N_SP, TOK_DEV, ATTENDER_TOTAL, HEAD_DIM)
    value = project(w_value).astype(jnp.bfloat16).reshape(N_SP, TOK_DEV, ATTENDER_TOTAL, HEAD_DIM)
    cum_blocks = cum_gate.reshape(ATTENDER_TOTAL, N_SP, TOK_DEV).transpose(1, 0, 2)

    def one_query_block(query_idx):
        q_blk = query[query_idx]
        q_cum = cum_blocks[query_idx]

        def visit(key_idx, state):
            terms = block_terms(q_blk, q_cum, key_rows[key_idx], value[key_idx], cum_blocks[key_idx], query_idx * TOK_DEV, key_idx * TOK_DEV)
            return merge_terms(state, terms)
        start_state = (jnp.full((ATTENDER_TOTAL, TOK_DEV), neg_large, jnp.float32), jnp.zeros((ATTENDER_TOTAL, TOK_DEV), jnp.float32), jnp.zeros((ATTENDER_TOTAL, TOK_DEV, HEAD_DIM), jnp.float32))
        top_all, total_all, acc_all = lax.fori_loop(0, query_idx + 1, visit, start_state)
        result = (acc_all / total_all[..., None]).transpose(1, 0, 2).reshape(TOK_DEV, ATT_W).astype(jnp.bfloat16)
        return (result, top_all + jnp.log(total_all))
    attn_blocks, log_blocks = lax.map(one_query_block, jnp.arange(N_SP, dtype=jnp.int32))
    attn_out = attn_blocks.reshape(SEQUENCE_SPAN, ATT_W)
    log_total = log_blocks.transpose(1, 0, 2).reshape(ATTENDER_TOTAL, SEQUENCE_SPAN)
    chan_group = CONV_CH // N_TP
    head_group = ATT_W // N_TP
    mixed = jnp.zeros((SEQUENCE_SPAN, D), jnp.float32)
    for group_idx in range(N_TP):
        part = jnp.dot(conv_out[:, group_idx * chan_group:(group_idx + 1) * chan_group], w_conv_out[group_idx * chan_group:(group_idx + 1) * chan_group], preferred_element_type=jnp.float32)
        part = part + jnp.dot(attn_out[:, group_idx * head_group:(group_idx + 1) * head_group], w_attn_out[group_idx * head_group:(group_idx + 1) * head_group], preferred_element_type=jnp.float32)
        part_round = lax.optimization_barrier(part.astype(jnp.bfloat16))
        mixed = mixed + part_round.astype(jnp.float32)
    return (mixed.astype(jnp.bfloat16), log_total)
```

```python
import functools
import jax
import jax.numpy as jnp
from jax import lax
from jax.experimental import pallas as pl
from jax.experimental.pallas import tpu as pltpu
from jax.sharding import PartitionSpec as P

D = 2048
CONV_CH = 1024
HEADS = 16


neg_large = -1e30


def passed_along(block, axis, distance):
    devices = range(lax.axis_size(axis))
    route = [(i - distance, i) for i in devices if i - distance in devices]
    return lax.ppermute(block, axis, route)


def block_terms(q_blk, q_cum, k_blk, v_blk, k_cum, q_first, k_first):
    score_scale = q_blk.shape[2] ** (-0.5)
    scores = (
        jnp.einsum("qhd,khd->hqk", q_blk, k_blk, preferred_element_type=jnp.float32) * score_scale
    )
    scores = scores + q_cum[:, :, None] - k_cum[:, None, :]
    q_pos = q_first + jnp.arange(q_blk.shape[0], dtype=jnp.int32)
    k_pos = k_first + jnp.arange(k_blk.shape[0], dtype=jnp.int32)
    allowed = k_pos[None, :] <= q_pos[:, None]
    scores = jnp.where(allowed[None], scores, -jnp.inf)
    block_top = jnp.max(scores, axis=-1)
    weights = jnp.exp(scores - block_top[..., None])
    block_total = jnp.sum(weights, axis=-1)
    block_out = jnp.einsum(
        "hqk,khd->hqd", weights.astype(jnp.bfloat16), v_blk, preferred_element_type=jnp.float32
    ).astype(jnp.bfloat16)
    return (block_top, block_total, block_out)


def merge_terms(state, terms):
    top_now, total_now, acc_now = state
    block_top, block_total, block_out = terms
    top_new = jnp.maximum(top_now, block_top)
    keep_old = jnp.exp(top_now - top_new)
    keep_new = jnp.exp(block_top - top_new)
    return (
        top_new,
        total_now * keep_old + block_total * keep_new,
        acc_now * keep_old[..., None] + block_out.astype(jnp.float32) * keep_new[..., None],
    )


def local(
    inputs,
    norm_gain,
    w_conv_in,
    w_conv_gate,
    conv_kernel,
    ln_gain,
    w_query,
    w_key,
    w_value,
    cum_gate,
    w_conv_out,
    w_attn_out,
):
    rows_here = inputs.shape[0]
    conv_width = w_conv_in.shape[0]
    attn_width = w_query.shape[0]
    heads_here = cum_gate.shape[0]
    head_dim = attn_width // heads_here
    taps_count = conv_kernel.shape[0]
    w_all = jnp.concatenate([w_conv_in, w_conv_gate, w_query, w_key, w_value], axis=0)
    gain_all = norm_gain.astype(jnp.float32)
    contract_dims = (((1,), (1,)), ((), ()))
    piece_f = lax.all_gather(inputs, "tp", axis=1, tiled=True).astype(jnp.float32)
    scaled_piece = (piece_f * gain_all[None, :]).astype(jnp.bfloat16)
    raw_proj = lax.dot_general(
        scaled_piece, w_all, contract_dims, preferred_element_type=jnp.float32
    )
    squares = jnp.sum(piece_f * piece_f, axis=1)
    rms = lax.rsqrt(squares / D + 1e-06)[:, None]
    proj = raw_proj * rms
    conv_in = proj[:, :conv_width]
    conv_gate = proj[:, conv_width : 2 * conv_width]
    query = proj[:, 2 * conv_width : 2 * conv_width + attn_width].astype(jnp.bfloat16)
    key_rows = proj[:, 2 * conv_width + attn_width : 2 * conv_width + 2 * attn_width].astype(
        jnp.bfloat16
    )
    value = proj[:, 2 * conv_width + 2 * attn_width :].astype(jnp.bfloat16)
    glu = (conv_in * jax.nn.sigmoid(conv_gate)).astype(jnp.bfloat16)
    rim_rows = passed_along(glu[rows_here - (taps_count - 1) :], "sp", 1)
    extended = jnp.concatenate([rim_rows, glu], axis=0)
    kernel = conv_kernel.astype(jnp.float32)
    conv_sum = jnp.zeros((rows_here, conv_width), jnp.float32)
    for tap_idx in range(taps_count):
        conv_sum = (
            conv_sum
            + extended[tap_idx : tap_idx + rows_here].astype(jnp.float32) * kernel[tap_idx][None, :]
        )
    chan_first, chan_second = lax.psum(
        (jnp.sum(conv_sum, axis=1), jnp.sum(conv_sum * conv_sum, axis=1)), "tp"
    )
    chan_mean = (chan_first / CONV_CH)[:, None]
    chan_var = (chan_second / CONV_CH)[:, None] - chan_mean * chan_mean
    normed = (
        (conv_sum - chan_mean) * lax.rsqrt(chan_var + 1e-05) * ln_gain.astype(jnp.float32)[None, :]
    )
    conv_out = jax.nn.silu(normed).astype(jnp.bfloat16)
    q_heads = query.reshape(rows_here, heads_here, head_dim)
    cum_all = lax.all_gather(cum_gate.T, "sp", axis=0, tiled=True)
    own_first = lax.axis_index("sp") * rows_here
    start_state = (
        jnp.full((heads_here, rows_here), neg_large, jnp.float32),
        jnp.zeros((heads_here, rows_here), jnp.float32),
        jnp.zeros((heads_here, rows_here, head_dim), jnp.float32),
    )
    state = start_state
    k_piece = lax.all_gather(key_rows, "sp", axis=0, tiled=True)
    v_piece = lax.all_gather(value, "sp", axis=0, tiled=True)
    block_count = k_piece.shape[0] // rows_here
    k_split = k_piece.reshape(block_count, rows_here, heads_here, head_dim)
    v_split = v_piece.reshape(block_count, rows_here, heads_here, head_dim)

    def visit(carry, item):
        k_blk, v_blk, block_idx = item
        k_first = block_idx * rows_here
        k_cum = lax.dynamic_slice_in_dim(cum_all, k_first, rows_here, 0).T

        def take_block(inner):
            return merge_terms(
                inner, block_terms(q_heads, cum_gate, k_blk, v_blk, k_cum, own_first, k_first)
            )

        def skip_block(inner):
            return inner

        return (lax.cond(k_first <= own_first, take_block, skip_block, carry), None)

    state, unused = lax.scan(
        visit, state, (k_split, v_split, jnp.arange(block_count, dtype=jnp.int32))
    )
    top_all, total_all, acc_all = state
    attn_out = (
        (acc_all / total_all[..., None])
        .transpose(1, 0, 2)
        .reshape(rows_here, attn_width)
        .astype(jnp.bfloat16)
    )
    log_total = top_all + jnp.log(total_all)
    mixed = lax.psum_scatter(
        (
            jnp.dot(conv_out, w_conv_out, preferred_element_type=jnp.float32)
            + jnp.dot(attn_out, w_attn_out, preferred_element_type=jnp.float32)
        ).astype(jnp.bfloat16),
        "tp",
        scatter_dimension=0,
        tiled=True,
    )
    return (mixed, log_total)


AG_CHUNKS = 4
OUT_CHUNKS = 4
MESH = pl.DeviceIdType.MESH
NT = (((1,), (1,)), ((), ()))
KV, Q = 0, 1
CROSS, SAME, OTHER = 0, 1, 2
ROUTES = (
    ((3, KV, 3, CROSS), (2, KV, 2, CROSS), (3, KV, 1, OTHER), (1, KV, 1, SAME)),
    ((3, KV, 3, CROSS), (2, KV, 2, CROSS), (0, KV, 0, CROSS), (2, Q, 0, OTHER), (0, Q, 0, SAME)),
    ((0, Q, 0, CROSS), (1, Q, 1, CROSS), (3, Q, 3, CROSS), (0, KV, 3, OTHER), (3, KV, 3, SAME)),
    ((0, Q, 0, CROSS), (1, Q, 1, CROSS), (1, Q, 2, OTHER), (2, Q, 2, SAME)),
)


def fused_kernel(n_tp, names, *refs):
    f32, bf16 = jnp.float32, jnp.bfloat16
    R = dict(zip(names, refs, strict=True))
    x_hbm, wci_hbm, wcg_hbm = R["x_hbm"], R["wci_hbm"], R["wcg_hbm"]
    wq_hbm, wk_hbm, wv_hbm = R["wq_hbm"], R["wk_hbm"], R["wv_hbm"]
    out_ref, log_ref = R["out_ref"], R["log_ref"]
    xg, xs, wbuf, wco, wao, acc, ss = (
        R[n] for n in ("xg", "xs", "wbuf", "wco", "wao", "acc", "ss")
    )
    gain_ref, ck_ref, lng_ref, cum_ref = R["gain"], R["ck"], R["lng"], R["cum"]
    zsend, zrecv, zx = R["zsend"], R["zrecv"], R["zx"]
    q_s, k_s, v_s, v_t = R["q_s"], R["k_s"], R["v_s"], R["v_t"]
    out_loc, lse_loc, cum_col, cum_recv = R["out_loc"], R["lse_loc"], R["cum_col"], R["cum_recv"]
    ext, halo_src, halo, csum = R["ext"], R["halo_src"], R["halo"], R["csum"]
    st_send, st_recv, cpart = R["st_send"], R["st_recv"], R["cpart"]
    t2_o, t2_l, q_cum = R["t2_o"], R["t2_l"], R["q_cum"]
    ret_send, ret_recv, lse_send, lse_recv = (
        R["ret_send"], R["ret_recv"], R["lse_send"], R["lse_recv"],
    )
    d_send, d_recv, x_send, x_recv, parts = (
        R[n] for n in ("d_send", "d_recv", "x_send", "x_recv", "parts")
    )
    ld = R["ld"]
    n_sp = len(ROUTES)
    z = lax.axis_index("sp")
    me = lax.axis_index("tp")
    chip, core = me // 2, me % 2
    chips = n_tp // 2
    rows, width = x_hbm.shape
    conv_w = wci_hbm.shape[0]
    attn_w = wq_hbm.shape[0]
    heads = n_sp
    hd = attn_w // heads
    d_all = wci_hbm.shape[1]
    partner = chip * 2 + 1 - core
    upper = z // 2
    z_near = z + 1 - 2 * (z % 2)
    key_blk, query_blk = 2 * upper, 2 * upper + 1
    other_head = (1 - upper) * (z + 2) + upper * (3 - z)

    def remote(src, dst, s, r, dev):
        return pltpu.make_async_remote_copy(
            src_ref=src, dst_ref=dst, send_sem=s, recv_sem=r, device_id=dev, device_id_type=MESH
        )

    def settle(ref, sem):
        pltpu.make_async_copy(ref, ref, sem).wait()

    def same_core(dist):
        return lax.rem(chip + dist, chips) * 2 + core

    def other_core(dist):
        return lax.rem(chip + dist, chips) * 2 + 1 - core

    def piece_owner(rel):
        return same_core(rel // 2) if rel % 2 == 0 else other_core(rel // 2)

    def piece_source(rel):
        back = chips - rel // 2
        return same_core(back) if rel % 2 == 0 else other_core(back)

    barrier = pltpu.get_barrier_semaphore()
    for rel in range(1, n_tp):
        pl.semaphore_signal(
            barrier, inc=1, device_id={"tp": piece_owner(rel)}, device_id_type=MESH
        )
    for dist in range(1, n_sp):
        pl.semaphore_signal(
            barrier, inc=1, device_id={"sp": lax.rem(z + dist, n_sp)}, device_id_type=MESH
        )

    own_copy = pltpu.make_async_copy(x_hbm, xg.at[0], ld.at[0])
    own_copy.start()
    small = [
        pltpu.make_async_copy(R[n + "_hbm"], R[n], ld.at[5 + i])
        for i, n in enumerate(("gain", "ck", "lng", "cum"))
    ]
    for c in small:
        c.start()
    qkv_w = 3 * attn_w
    own_copy.wait()
    for h in range(heads):
        for i, w in enumerate((wk_hbm, wv_hbm)):
            pltpu.make_async_copy(
                w.at[pl.ds(h * hd, hd)], wbuf.at[pl.ds((2 * h + i) * hd, hd)], ld.at[1]
            ).start()
    pltpu.make_async_copy(wq_hbm, wbuf.at[pl.ds(2 * attn_w, attn_w)], ld.at[1]).start()
    pltpu.make_async_copy(wci_hbm, wbuf.at[pl.ds(qkv_w, conv_w)], ld.at[2]).start()
    pltpu.make_async_copy(wcg_hbm, wbuf.at[pl.ds(qkv_w + conv_w, conv_w)], ld.at[2]).start()
    wco_copy = pltpu.make_async_copy(R["wco_hbm"], wco, ld.at[3])
    wao_copy = pltpu.make_async_copy(R["wao_hbm"], wao, ld.at[4])
    wco_copy.start()
    wao_copy.start()

    pl.semaphore_wait(barrier, n_tp - 1 + n_sp - 1)

    rc = rows // AG_CHUNKS

    def ag_copy(rel, relay, c):
        r = pl.ds(c * rc, rc)
        src, to = (xg.at[rel - 1, r], partner) if relay else (xg.at[0, r], piece_owner(rel))
        return remote(src, xg.at[rel, r], R["ag_s"], R["ag_r"].at[rel - 2, c], {"tp": to})

    order = [AG_CHUNKS - 1] + list(range(AG_CHUNKS - 1))
    for c in order:
        for dist in range(1, chips):
            ag_copy(2 * dist, False, c).start()
    pair_copy = remote(xg.at[0], xg.at[1], R["ag_s"], R["ag_r1"], {"tp": partner})
    pair_copy.start()
    small[3].wait()
    for dist in range(1, n_sp):
        remote(
            cum_ref, cum_recv.at[z], R["cs"], R["cr"], {"sp": lax.rem(z + dist, n_sp)}
        ).start()
    cum_recv[z] = cum_ref[...]
    small[0].wait()

    def prepare(rel, c0, n):
        r = pl.ds(c0, n)
        owner = piece_source(rel)
        raw = xg[rel, r].astype(f32)
        g = gain_ref[pl.ds(pl.multiple_of(owner * width, width), width)].astype(f32).reshape(1, width)
        xs[rel, r] = (raw * g).astype(bf16)
        return jnp.sum(raw * raw, axis=1, keepdims=True)

    def wcols(rel, first, n):
        owner = piece_source(rel)
        return wbuf[pl.ds(first, n), pl.ds(pl.multiple_of(owner * width, width), width)]

    ss[...] = prepare(0, 0, rows)
    settle(wbuf.at[pl.ds(0, qkv_w)], ld.at[1])
    acc[:, :qkv_w] = lax.dot_general(xs[0], wcols(0, 0, qkv_w), NT, preferred_element_type=f32)
    settle(wbuf.at[pl.ds(qkv_w, 2 * conv_w)], ld.at[2])
    acc[:, qkv_w:] = lax.dot_general(
        xs[0], wcols(0, qkv_w, 2 * conv_w), NT, preferred_element_type=f32
    )
    pair_copy.wait_recv()
    ss[...] += prepare(1, 0, rows)
    acc[...] += lax.dot_general(
        xs[1], wcols(1, 0, qkv_w + 2 * conv_w), NT, preferred_element_type=f32
    )

    half = rc // 2
    spans = (pl.ds(0, rc), pl.ds(rc, half))

    def finish_chunk(c):
        r = pl.ds(c * rc, rc)
        total = acc[r, :qkv_w]
        sq = ss[r]
        for dist in range(1, chips):
            ag_copy(2 * dist + 1, True, c).wait_recv()
            sq = sq + prepare(2 * dist + 1, c * rc, rc)
            total = total + lax.dot_general(
                xs[2 * dist + 1, r],
                wcols(2 * dist + 1, 0, qkv_w),
                NT,
                preferred_element_type=f32,
            )
        rms = lax.rsqrt(sq / d_all + 1e-06)
        ss[r] = rms
        total = total * rms
        for h in range(heads):
            zsend[h, c, :rc] = total[:, 2 * h * hd : 2 * (h + 1) * hd].astype(bf16)
            q_h = total[:, 2 * attn_w + h * hd : 2 * attn_w + (h + 1) * hd]
            zsend[h, c, rc:] = jnp.concatenate([q_h[:half], q_h[half:]], axis=1).astype(bf16)
        for src, routes in enumerate(ROUTES):

            @pl.when(z == src)
            def _():
                for h, part, to, kind in routes:
                    dst = zx.at[c, spans[part]] if kind == OTHER else zrecv.at[src, c, spans[part]]
                    remote(
                        zsend.at[h, c, spans[part]], dst, R["zs"], R["zr"].at[kind], {"sp": to}
                    ).start()

        zrecv[z, c] = zsend[z, c]

        @pl.when(z % 2 == 0)
        def _():
            zx[c, :rc] = zsend[other_head, c, :rc]

        @pl.when(z % 2 == 1)
        def _():
            zx[c, rc:] = zsend[other_head, c, rc:]

    rim = halo.shape[0]
    halo_copy = remote(halo_src, halo, R["hs"], R["hr"], {"sp": lax.rem(z + 1, n_sp)})

    def gated(r):
        pre = acc[r, qkv_w:]
        for rel in range(2, n_tp):
            pre = pre + lax.dot_general(
                xs[rel, r], wcols(rel, qkv_w, 2 * conv_w), NT, preferred_element_type=f32
            )
        pre = pre * ss[r]
        return (pre[:, :conv_w] * jax.nn.sigmoid(pre[:, conv_w:])).astype(bf16)

    for k, c in enumerate(order):
        r = pl.ds(c * rc, rc)
        for dist in range(1, chips):
            ag_copy(2 * dist, False, c).wait_recv()
            ag_copy(2 * dist + 1, True, c).start()
        for dist in range(1, chips):
            ss[r] += prepare(2 * dist, c * rc, rc)
            acc[r, :qkv_w] += lax.dot_general(
                xs[2 * dist, r], wcols(2 * dist, 0, qkv_w), NT, preferred_element_type=f32
            )
        if k == 0:
            finish_chunk(c)
        elif k == 1:
            halo_src[...] = gated(pl.ds(rows - rim, rim))

            @pl.when(z < n_sp - 1)
            def _():
                halo_copy.start()

        else:
            finish_chunk(order[k - 1])
    finish_chunk(order[-1])

    glu = gated(pl.ds(0, rows))
    taps = ck_ref.shape[0]
    ext[rim:, :] = glu.astype(f32)
    blk = 64
    small[1].wait()
    small[2].wait()

    def conv_block(b, carry):
        first = pl.multiple_of(b * blk, blk)
        block = ext[pl.ds(first, blk + rim), :]
        tot = jnp.zeros((blk, conv_w), f32)
        for j in range(taps):
            off = rim - (taps - 1) + j
            tot = tot + block[off : off + blk] * ck_ref[j : j + 1, :].astype(f32)
        csum[pl.ds(first, blk), :] = tot
        return carry

    lax.fori_loop(1, rows // blk, conv_block, 0)
    settle(cum_recv.at[pl.ds(0, n_sp - 1)], R["cr"])
    for i, (src, h) in enumerate(((0, z), (1, z), (key_blk, z), (key_blk, other_head))):
        cum_col[pl.ds(i * rows, rows)] = jnp.broadcast_to(
            cum_recv[src, pl.ds(h, 1)], (128, rows)
        ).T

    @pl.when(z == 0)
    def _():
        halo[...] = jnp.zeros_like(halo)

    @pl.when(z > 0)
    def _():
        halo_copy.wait_recv()

    ext[:rim, :] = halo[...].astype(f32)
    conv_block(0, 0)
    cs = csum[...]
    first = jnp.sum(cs, axis=1, keepdims=True)
    second = jnp.sum(cs * cs, axis=1, keepdims=True)
    lane = lax.broadcasted_iota(jnp.int32, (rows, 128), 1)
    both = jnp.where(lane == 0, first, second)
    st_send[...] = both.T[: st_send.shape[0]]
    for rel in range(1, n_tp):
        remote(
            st_send, st_recv.at[rel - 1], R["st_s"], R["st_r"], {"tp": piece_owner(rel)}
        ).start()
    scale = hd ** (-0.5)
    low = lax.broadcasted_iota(jnp.int32, (rc, 2 * hd), 1) < hd
    wide_k = -(-rows // 128)
    allowed = lax.broadcasted_iota(jnp.int32, (rows, rows), 0) <= lax.broadcasted_iota(
        jnp.int32, (rows, rows), 1
    )

    def take_keys(tile, r0):
        kv = tile.astype(f32)
        k_s[pl.ds(r0, rc)] = kv[:, :hd].astype(bf16)
        v_s[pl.ds(r0, rc)] = jnp.where(low, pltpu.roll(kv, hd, 1), 1.0).astype(bf16)

    def take_queries(tile, r0):
        qt = tile.astype(f32) * scale
        q_s[pl.ds(r0, half)] = qt[:, :hd].astype(bf16)
        q_s[pl.ds(r0 + half, half)] = qt[:, hd:].astype(bf16)

    def attend(q, k, vt, cum_k, causal):
        sc = lax.dot_general(k, q, NT, preferred_element_type=f32) - cum_k
        if causal:
            sc = jnp.where(allowed, sc, -jnp.inf)
        top = jnp.max(sc, axis=0, keepdims=True)
        p = jnp.exp(sc - top).astype(bf16)
        both = jnp.dot(vt, p, preferred_element_type=f32)
        tot = both[hd : hd + 1]
        return both[:hd] / tot, top + jnp.log(tot)

    for h in range(heads):
        for c in range(AG_CHUNKS):
            take_keys(zsend[h, c, :rc], h * rows + c * rc)
            take_queries(zsend[h, c, rc:], h * rows + c * rc)
    v_t[...] = v_s[...].T
    for h in range(heads):
        own = pl.ds(h * rows, rows)
        own_cum = cum_ref[pl.ds(h, 1), :]
        col = jnp.broadcast_to(own_cum, (128, rows)).T
        out_loc[pl.ds(h * hd, hd), :], lse = attend(
            q_s[own], k_s[own], v_t[:, h * rows : (h + 1) * rows],
            jnp.concatenate([col] * wide_k, axis=1), True,
        )
        lse_loc[pl.ds(h, 1), :] = lse + own_cum

    qk_rows = half * 2 * hd * AG_CHUNKS // width

    def arrived(kind, units):
        for src, n in enumerate(units):

            @pl.when(z == src)
            def _():
                settle(xs.at[0, pl.ds(0, n * qk_rows)], R["zr"].at[kind])

    own_rows = rows // n_tp
    chip_rows = 2 * own_rows
    lanes = [
        pl.ds(pl.multiple_of(lax.rem(chip + 1 + i, chips) * chip_rows, chip_rows), chip_rows)
        for i in range(chips)
    ]

    def send_back(src_o, dst_o, src_l, dst_l, kind, to):
        remote(src_o, dst_o, R["rs"], R["rr"].at[kind], {"sp": to}).start()
        remote(src_l, dst_l, R["ls"], R["lr"].at[kind], {"sp": to}).start()

    arrived(OTHER, (1, 2, 1, 2))
    for c in range(AG_CHUNKS):
        take_keys(zx[c, :rc], c * rc)
        take_queries(zx[c, rc:], c * rc)
    v_t[:, :rows] = v_s[:rows].T
    o, lse = attend(
        q_s[:rows], k_s[:rows], v_t[:, :rows],
        jnp.concatenate([cum_col[3 * rows :]] * wide_k, axis=1), False,
    )
    lse = lse + cum_recv[query_blk, pl.ds(other_head, 1)]
    t2_o[...] = o
    t2_l[...] = lse
    slot = other_head + 4 * upper
    for i in range(chips):
        ret_send[3, i] = t2_o[:, lanes[i]].astype(bf16)
        lse_send[3, i] = t2_l[:, lanes[i]]

    @pl.when(z % 2 == 0)
    def _():
        send_back(
            ret_send.at[3], ret_recv.at[slot], lse_send.at[3], lse_recv.at[slot], 2, z + 1
        )

    @pl.when(z % 2 == 1)
    def _():
        ret_recv[slot] = ret_send[3]
        lse_recv[slot] = lse_send[3]

    arrived(SAME, (1, 2, 1, 2))
    for c in range(AG_CHUNKS):
        take_keys(zrecv[key_blk, c, :rc], c * rc)
        take_queries(zrecv[query_blk, c, rc:], c * rc)
    v_t[:, :rows] = v_s[:rows].T
    o, lse = attend(
        q_s[:rows], k_s[:rows], v_t[:, :rows],
        jnp.concatenate([cum_col[2 * rows : 3 * rows]] * wide_k, axis=1), False,
    )
    lse = lse + cum_recv[query_blk, pl.ds(z, 1)]
    t2_o[...] = o
    t2_l[...] = lse
    for i in range(chips):
        ret_send[2, i] = t2_o[:, lanes[i]].astype(bf16)
        lse_send[2, i] = t2_l[:, lanes[i]]

    @pl.when(z == 0)
    def _():
        send_back(ret_send.at[2], ret_recv.at[z], lse_send.at[2], lse_recv.at[z], 2, 1)

    @pl.when(z == 1)
    def _():
        ret_recv[z] = ret_send[2]
        lse_recv[z] = lse_send[2]

    settle(st_recv, R["st_r"])
    tot = st_send[...]
    for rel in range(1, n_tp):
        tot = tot + st_recv[rel - 1]
    wide = jnp.concatenate([tot] * (128 // tot.shape[0]), axis=0).T
    mean = wide[:, 0:1] / CONV_CH
    var = wide[:, 1:2] / CONV_CH - mean * mean
    normed = (csum[...] - mean) * lax.rsqrt(var + 1e-05) * lng_ref[...].astype(f32).reshape(1, conv_w)
    conv_out = (normed / (1.0 + jnp.exp(-normed))).astype(bf16)
    wco_copy.wait()
    cpart[...] = jnp.dot(conv_out, wco[...], preferred_element_type=f32)

    arrived(CROSS, (4, 2, 4, 5))
    for b in range(2):
        for c in range(AG_CHUNKS):
            take_keys(zrecv[b, c, :rc], b * rows + c * rc)
            take_queries(zrecv[2 + b, c, rc:], b * rows + c * rc)
    v_t[:, : 2 * rows] = v_s[: 2 * rows].T
    for b in range(2):
        q_cum[b : b + 1] = cum_recv[2 + b, pl.ds(z, 1)]
    for i in range(chips):
        q = jnp.concatenate(
            [
                q_s[pl.ds(pl.multiple_of(b * rows + lanes[i].start, chip_rows), chip_rows)]
                for b in range(2)
            ],
            axis=0,
        )
        o, lse = attend(
            q, k_s[: 2 * rows], v_t[:, : 2 * rows],
            jnp.concatenate([cum_col[: 2 * rows]] * (2 * chip_rows // 128), axis=1), False,
        )
        for b in range(2):
            o_b = o[:, b * chip_rows : (b + 1) * chip_rows]
            lse_b = lse[:, b * chip_rows : (b + 1) * chip_rows]
            lse_b = lse_b + q_cum[b : b + 1, lanes[i]]
            if b == 1:
                lse_n = jnp.where(upper == 1, t2_l[:, lanes[i]], neg_large)
                top = jnp.maximum(lse_b, lse_n)
                w_b, w_n = jnp.exp(lse_b - top), jnp.exp(lse_n - top)
                tot = w_b + w_n
                o_b = (o_b * w_b + t2_o[:, lanes[i]] * w_n) / tot
                lse_b = top + jnp.log(tot)
            ret_send[b, i] = o_b.astype(bf16)
            lse_send[b, i] = lse_b
        for b in range(1, -1, -1):

            @pl.when(z != 2 + b)
            def _():
                send_back(
                    ret_send.at[b, i], ret_recv.at[z, i],
                    lse_send.at[b, i], lse_recv.at[z, i], i, 2 + b,
                )

            @pl.when(z == 2 + b)
            def _():
                ret_recv[z, i] = ret_send[b, i]
                lse_recv[z, i] = lse_send[b, i]

    def merge(h, slot, i):
        r = pl.ds(h * hd, hd)
        near, far = lse_loc[pl.ds(h, 1), lanes[i]], lse_recv[slot, i]
        top = jnp.maximum(near, far)
        w_near, w_far = jnp.exp(near - top), jnp.exp(far - top)
        tot = w_near + w_far
        out_loc[r, lanes[i]] = (
            out_loc[r, lanes[i]] * w_near + ret_recv[slot, i].astype(f32) * w_far
        ) / tot
        lse_loc[pl.ds(h, 1), lanes[i]] = top + jnp.log(tot)

    @pl.when(z == 1)
    def _():
        settle(ret_recv.at[pl.ds(0, 2)], R["rr"].at[2])
        settle(lse_recv.at[pl.ds(0, 2)], R["lr"].at[2])
        for i in range(chips):
            for h in range(heads):
                merge(h, h, i)

    @pl.when(z == 3)
    def _():
        settle(ret_recv.at[pl.ds(0, 1)], R["rr"].at[2])
        settle(lse_recv.at[pl.ds(0, 1)], R["lr"].at[2])
        for i in range(chips):
            for h in range(2):
                merge(h, 4 + h, i)

    wao_copy.wait()
    cw = d_all // OUT_CHUNKS
    mine = pl.ds(pl.multiple_of(core * own_rows, own_rows), own_rows)
    theirs = pl.ds(pl.multiple_of((1 - core) * own_rows, own_rows), own_rows)

    def d_copy(dist, n):
        return remote(
            d_send.at[dist, n], d_recv.at[dist, n], R["ds"], R["dr"].at[dist, n], {"tp": partner}
        )

    def x_copy(n):
        return remote(x_send.at[n], x_recv.at[n], R["xs_s"], R["xr"].at[n], {"tp": same_core(1)})

    def exchange(dist):
        i = chips - 1 - dist

        @pl.when(z > 1)
        def _():
            settle(ret_recv.at[pl.ds(0, 3), i], R["rr"].at[i])
            settle(lse_recv.at[pl.ds(0, 3), i], R["lr"].at[i])
            for h in range(heads):
                merge(h, h, i)

        att = out_loc[:, lanes[i]].T.astype(bf16)
        for n in range(OUT_CHUNKS):
            cols = slice(n * cw, (n + 1) * cw)
            parts[dist, n] = cpart[lanes[i], cols] + jnp.dot(
                att, wao[:, cols], preferred_element_type=f32
            )
            d_send[dist, n] = parts[dist, n, theirs].astype(bf16)
            d_copy(dist, n).start()

    exchange(1)
    for n in range(OUT_CHUNKS):
        d_copy(1, n).wait_recv()
        x_send[n] = (parts[1, n, mine] + d_recv[1, n].astype(f32)).astype(bf16)
        x_copy(n).start()
    exchange(0)
    log_ref[...] = lse_loc[...]
    for n in range(OUT_CHUNKS):
        d_copy(0, n).wait_recv()
        tot = parts[0, n, mine] + d_recv[0, n].astype(f32)
        x_copy(n).wait_recv()
        tot = tot + x_recv[n].astype(f32)
        out_ref[:, n * cw : (n + 1) * cw] = tot.astype(bf16)

    settle(xg.at[pl.ds(1, n_tp - 1)], R["ag_s"])
    settle(cum_recv.at[pl.ds(0, n_sp - 1)], R["cs"])
    settle(st_recv, R["st_s"])
    settle(d_send, R["ds"])
    settle(x_send, R["xs_s"])

    @pl.when(z < n_sp - 1)
    def _():
        halo_copy.wait_send()

    sent = [sum(2 if r[1] == KV else 1 for r in routes) for routes in ROUTES]
    for src, (n, back) in enumerate(zip(sent, (4, 2, 2, 1), strict=True)):

        @pl.when(z == src)
        def _():
            settle(xs.at[0, pl.ds(0, n * qk_rows)], R["zs"])
            settle(ret_recv.at[pl.ds(0, back)], R["rs"])
            settle(lse_recv.at[pl.ds(0, back)], R["ls"])


def write_out(m_ref, l_ref, m_hbm, l_hbm, sem):
    a = pltpu.make_async_copy(m_ref, m_hbm, sem.at[0])
    b = pltpu.make_async_copy(l_ref, l_hbm, sem.at[1])
    a.start()
    b.start()
    a.wait()
    b.wait()


ARGS = (
    "x_hbm", "gain_hbm", "wci_hbm", "wcg_hbm", "ck_hbm", "lng_hbm",
    "wq_hbm", "wk_hbm", "wv_hbm", "cum_hbm", "wco_hbm", "wao_hbm",
)


def fused_local(n_tp, *args):
    f32, bf16 = jnp.float32, jnp.bfloat16
    inputs, norm_gain, w_conv_in, _, conv_kernel, ln_gain, w_query, _, _, cum_gate, _, _ = args
    n_sp = len(ROUTES)
    rows, width = inputs.shape
    conv_w, d_all = w_conv_in.shape
    attn_w = w_query.shape[0]
    heads = cum_gate.shape[0]
    hd = attn_w // heads
    chips = n_tp // 2
    own_rows = rows // n_tp
    rc = rows // AG_CHUNKS
    rim = -(-(conv_kernel.shape[0] - 1) // 16) * 16
    cw = d_all // OUT_CHUNKS
    all_w = 3 * attn_w + 2 * conv_w
    dma = pltpu.SemaphoreType.DMA
    vm = pltpu.VMEM
    scratch = {
        "xg": vm((n_tp, rows, width), bf16),
        "xs": vm((n_tp, rows, width), bf16),
        "wbuf": vm((all_w, d_all), bf16),
        "wco": vm((conv_w, d_all), bf16),
        "wao": vm((attn_w, d_all), bf16),
        "gain": vm(norm_gain.shape, bf16),
        "ck": vm(conv_kernel.shape, bf16),
        "lng": vm(ln_gain.shape, bf16),
        "cum": vm(cum_gate.shape, f32),
        "acc": vm((rows, all_w), f32),
        "ss": vm((rows, 1), f32),
        "zsend": vm((n_sp, AG_CHUNKS, rc + rc // 2, 2 * hd), bf16),
        "zrecv": vm((n_sp, AG_CHUNKS, rc + rc // 2, 2 * hd), bf16),
        "zx": vm((AG_CHUNKS, rc + rc // 2, 2 * hd), bf16),
        "q_s": vm((n_sp * rows, hd), bf16),
        "k_s": vm((n_sp * rows, hd), bf16),
        "v_s": vm((n_sp * rows, 2 * hd), bf16),
        "v_t": vm((2 * hd, n_sp * rows), bf16),
        "out_loc": vm((attn_w, rows), f32),
        "lse_loc": vm((heads, rows), f32),
        "cum_col": vm((4 * rows, 128), f32),
        "cum_recv": vm((n_sp, heads, rows), f32),
        "ext": vm((rows + rim, conv_w), f32),
        "halo_src": vm((rim, conv_w), bf16),
        "halo": vm((rim, conv_w), bf16),
        "csum": vm((rows, conv_w), f32),
        "st_send": vm((8, rows), f32),
        "st_recv": vm((n_tp - 1, 8, rows), f32),
        "cpart": vm((rows, d_all), f32),
        "t2_o": vm((hd, rows), f32),
        "t2_l": vm((1, rows), f32),
        "q_cum": vm((2, rows), f32),
        "ret_send": vm((4, chips, hd, 2 * own_rows), bf16),
        "ret_recv": vm((6, chips, hd, 2 * own_rows), bf16),
        "lse_send": vm((4, chips, 1, 2 * own_rows), f32),
        "lse_recv": vm((6, chips, 1, 2 * own_rows), f32),
        "d_send": vm((chips, OUT_CHUNKS, own_rows, cw), bf16),
        "d_recv": vm((chips, OUT_CHUNKS, own_rows, cw), bf16),
        "x_send": vm((OUT_CHUNKS, own_rows, cw), bf16),
        "x_recv": vm((OUT_CHUNKS, own_rows, cw), bf16),
        "parts": vm((chips, OUT_CHUNKS, 2 * own_rows, cw), f32),
        "ld": dma((9,)),
        "ag_s": dma,
        "ag_r1": dma,
        "ag_r": dma((n_tp - 2, AG_CHUNKS)),
        "zs": dma,
        "zr": dma((3,)),
        "cs": dma,
        "cr": dma,
        "hs": dma,
        "hr": dma,
        "st_s": dma,
        "st_r": dma,
        "rs": dma,
        "ls": dma,
        "rr": dma((3,)),
        "lr": dma((3,)),
        "ds": dma,
        "dr": dma((chips, OUT_CHUNKS)),
        "xs_s": dma,
        "xr": dma((OUT_CHUNKS,)),
    }
    far = pl.BlockSpec(memory_space=pl.ANY)
    near = pl.BlockSpec(memory_space=pltpu.VMEM)
    results = pl.pallas_call(
        functools.partial(fused_kernel, n_tp, ARGS + ("out_ref", "log_ref") + tuple(scratch)),
        out_shape=(
            pltpu.VMEM((own_rows, d_all), bf16),
            pltpu.VMEM((heads, rows), f32),
        ),
        in_specs=[far] * len(ARGS),
        out_specs=(near, near),
        scratch_shapes=list(scratch.values()),
        compiler_params=pltpu.CompilerParams(
            collective_id=0, has_side_effects=True, vmem_limit_bytes=60 * 1024 * 1024
        ),
    )(*args)
    return pl.pallas_call(
        write_out,
        out_shape=(
            jax.ShapeDtypeStruct((own_rows, d_all), bf16),
            jax.ShapeDtypeStruct((heads, rows), f32),
        ),
        in_specs=[near, near],
        out_specs=(far, far),
        scratch_shapes=[dma((2,))],
    )(*[pltpu.with_memory_space_constraint(r, pltpu.VMEM) for r in results])


def solution(mesh):
    in_specs = (
        P(("grp", "sp"), "tp"),
        P(),
        P("tp", None),
        P("tp", None),
        P(None, "tp"),
        P("tp"),
        P("tp", None),
        P("tp", None),
        P("tp", None),
        P("tp", ("grp", "sp")),
        P("tp", None),
        P("tp", None),
    )
    out_specs = (P(("grp", "sp", "tp"), None), P("tp", ("grp", "sp")))
    heads_here = HEADS // mesh.shape["tp"]
    fits = heads_here == mesh.shape["sp"] == len(ROUTES) and mesh.shape["tp"] == 4
    body = functools.partial(fused_local, mesh.shape["tp"]) if fits else local
    return jax.shard_map(body, mesh=mesh, in_specs=in_specs, out_specs=out_specs, check_vma=False)
```

```python
import functools
import jax
import jax.numpy as jnp
from jax import lax
from jax.experimental import pallas as pl
from jax.experimental.pallas import tpu as pltpu
from jax.sharding import PartitionSpec as P

D = 2048
CONV_CH = 1024
HEADS = 16


neg_large = -1e30


def passed_along(block, axis, distance):
    devices = range(lax.axis_size(axis))
    route = [(i - distance, i) for i in devices if i - distance in devices]
    return lax.ppermute(block, axis, route)


def block_terms(q_blk, q_cum, k_blk, v_blk, k_cum, q_first, k_first):
    score_scale = q_blk.shape[2] ** (-0.5)
    scores = (
        jnp.einsum("qhd,khd->hqk", q_blk, k_blk, preferred_element_type=jnp.float32) * score_scale
    )
    scores = scores + q_cum[:, :, None] - k_cum[:, None, :]
    q_pos = q_first + jnp.arange(q_blk.shape[0], dtype=jnp.int32)
    k_pos = k_first + jnp.arange(k_blk.shape[0], dtype=jnp.int32)
    allowed = k_pos[None, :] <= q_pos[:, None]
    scores = jnp.where(allowed[None], scores, -jnp.inf)
    block_top = jnp.max(scores, axis=-1)
    weights = jnp.exp(scores - block_top[..., None])
    block_total = jnp.sum(weights, axis=-1)
    block_out = jnp.einsum(
        "hqk,khd->hqd", weights.astype(jnp.bfloat16), v_blk, preferred_element_type=jnp.float32
    ).astype(jnp.bfloat16)
    return (block_top, block_total, block_out)


def merge_terms(state, terms):
    top_now, total_now, acc_now = state
    block_top, block_total, block_out = terms
    top_new = jnp.maximum(top_now, block_top)
    keep_old = jnp.exp(top_now - top_new)
    keep_new = jnp.exp(block_top - top_new)
    return (
        top_new,
        total_now * keep_old + block_total * keep_new,
        acc_now * keep_old[..., None] + block_out.astype(jnp.float32) * keep_new[..., None],
    )


def local(
    inputs,
    norm_gain,
    w_conv_in,
    w_conv_gate,
    conv_kernel,
    ln_gain,
    w_query,
    w_key,
    w_value,
    cum_gate,
    w_conv_out,
    w_attn_out,
):
    rows_here = inputs.shape[0]
    conv_width = w_conv_in.shape[0]
    attn_width = w_query.shape[0]
    heads_here = cum_gate.shape[0]
    head_dim = attn_width // heads_here
    taps_count = conv_kernel.shape[0]
    w_all = jnp.concatenate([w_conv_in, w_conv_gate, w_query, w_key, w_value], axis=0)
    gain_all = norm_gain.astype(jnp.float32)
    contract_dims = (((1,), (1,)), ((), ()))
    piece_f = lax.all_gather(inputs, "tp", axis=1, tiled=True).astype(jnp.float32)
    scaled_piece = (piece_f * gain_all[None, :]).astype(jnp.bfloat16)
    raw_proj = lax.dot_general(
        scaled_piece, w_all, contract_dims, preferred_element_type=jnp.float32
    )
    squares = jnp.sum(piece_f * piece_f, axis=1)
    rms = lax.rsqrt(squares / D + 1e-06)[:, None]
    proj = raw_proj * rms
    conv_in = proj[:, :conv_width]
    conv_gate = proj[:, conv_width : 2 * conv_width]
    query = proj[:, 2 * conv_width : 2 * conv_width + attn_width].astype(jnp.bfloat16)
    key_rows = proj[:, 2 * conv_width + attn_width : 2 * conv_width + 2 * attn_width].astype(
        jnp.bfloat16
    )
    value = proj[:, 2 * conv_width + 2 * attn_width :].astype(jnp.bfloat16)
    glu = (conv_in * jax.nn.sigmoid(conv_gate)).astype(jnp.bfloat16)
    rim_rows = passed_along(glu[rows_here - (taps_count - 1) :], "sp", 1)
    extended = jnp.concatenate([rim_rows, glu], axis=0)
    kernel = conv_kernel.astype(jnp.float32)
    conv_sum = jnp.zeros((rows_here, conv_width), jnp.float32)
    for tap_idx in range(taps_count):
        conv_sum = (
            conv_sum
            + extended[tap_idx : tap_idx + rows_here].astype(jnp.float32) * kernel[tap_idx][None, :]
        )
    chan_first, chan_second = lax.psum(
        (jnp.sum(conv_sum, axis=1), jnp.sum(conv_sum * conv_sum, axis=1)), "tp"
    )
    chan_mean = (chan_first / CONV_CH)[:, None]
    chan_var = (chan_second / CONV_CH)[:, None] - chan_mean * chan_mean
    normed = (
        (conv_sum - chan_mean) * lax.rsqrt(chan_var + 1e-05) * ln_gain.astype(jnp.float32)[None, :]
    )
    conv_out = jax.nn.silu(normed).astype(jnp.bfloat16)
    q_heads = query.reshape(rows_here, heads_here, head_dim)
    cum_all = lax.all_gather(cum_gate.T, "sp", axis=0, tiled=True)
    own_first = lax.axis_index("sp") * rows_here
    start_state = (
        jnp.full((heads_here, rows_here), neg_large, jnp.float32),
        jnp.zeros((heads_here, rows_here), jnp.float32),
        jnp.zeros((heads_here, rows_here, head_dim), jnp.float32),
    )
    state = start_state
    k_piece = lax.all_gather(key_rows, "sp", axis=0, tiled=True)
    v_piece = lax.all_gather(value, "sp", axis=0, tiled=True)
    block_count = k_piece.shape[0] // rows_here
    k_split = k_piece.reshape(block_count, rows_here, heads_here, head_dim)
    v_split = v_piece.reshape(block_count, rows_here, heads_here, head_dim)

    def visit(carry, item):
        k_blk, v_blk, block_idx = item
        k_first = block_idx * rows_here
        k_cum = lax.dynamic_slice_in_dim(cum_all, k_first, rows_here, 0).T

        def take_block(inner):
            return merge_terms(
                inner, block_terms(q_heads, cum_gate, k_blk, v_blk, k_cum, own_first, k_first)
            )

        def skip_block(inner):
            return inner

        return (lax.cond(k_first <= own_first, take_block, skip_block, carry), None)

    state, unused = lax.scan(
        visit, state, (k_split, v_split, jnp.arange(block_count, dtype=jnp.int32))
    )
    top_all, total_all, acc_all = state
    attn_out = (
        (acc_all / total_all[..., None])
        .transpose(1, 0, 2)
        .reshape(rows_here, attn_width)
        .astype(jnp.bfloat16)
    )
    log_total = top_all + jnp.log(total_all)
    mixed = lax.psum_scatter(
        (
            jnp.dot(conv_out, w_conv_out, preferred_element_type=jnp.float32)
            + jnp.dot(attn_out, w_attn_out, preferred_element_type=jnp.float32)
        ).astype(jnp.bfloat16),
        "tp",
        scatter_dimension=0,
        tiled=True,
    )
    return (mixed, log_total)


AG_CHUNKS = 4
OUT_CHUNKS = 4
MESH = pl.DeviceIdType.MESH
NT = (((1,), (1,)), ((), ()))
KV, Q = 0, 1
CROSS, SAME, OTHER = 0, 1, 2
ROUTES = (
    ((3, KV, 3, CROSS), (2, KV, 2, CROSS), (1, KV, 1, SAME), (3, KV, 1, OTHER)),
    ((3, KV, 3, CROSS), (2, KV, 2, CROSS), (0, KV, 0, CROSS), (0, Q, 0, SAME), (2, Q, 0, OTHER)),
    ((0, Q, 0, CROSS), (1, Q, 1, CROSS), (3, Q, 3, CROSS), (3, KV, 3, SAME), (0, KV, 3, OTHER)),
    ((0, Q, 0, CROSS), (1, Q, 1, CROSS), (2, Q, 2, SAME), (1, Q, 2, OTHER)),
)
OTHER_HEAD = (2, 3, 1, 0)
TASKS = (
    ((CROSS, 0), (SAME, 0), (OTHER, 0)),
    ((CROSS, 0), (SAME, 0), (OTHER, 0), (CROSS, 1)),
    ((SAME, 0), (OTHER, 0), (CROSS, 0), (CROSS, 1)),
    ((SAME, 0), (OTHER, 0), (CROSS, 0), (CROSS, 1)),
)
LATE_TASKS = (((CROSS, 1),), (), (), ())
ROW_GROUPS = ((3,), (0,), (1, 2))


def fused_kernel(n_tp, names, *refs):
    f32, bf16 = jnp.float32, jnp.bfloat16
    R = dict(zip(names, refs, strict=True))
    x_hbm, wci_hbm, wcg_hbm = R["x_hbm"], R["wci_hbm"], R["wcg_hbm"]
    wq_hbm, wk_hbm, wv_hbm = R["wq_hbm"], R["wk_hbm"], R["wv_hbm"]
    out_ref, log_ref = R["out_ref"], R["log_ref"]
    xg, xs, wbuf, wco, wao, acc, ss = (
        R[n] for n in ("xg", "xs", "wbuf", "wco", "wao", "acc", "ss")
    )
    gain_ref, ck_ref, lng_ref, cum_ref = R["gain"], R["ck"], R["lng"], R["cum"]
    zsend, zrecv, zx = R["zsend"], R["zrecv"], R["zx"]
    q_s, k_s, v_s, v_t = R["q_s"], R["k_s"], R["v_s"], R["v_t"]
    out_loc, lse_loc, cum_col, cum_recv = R["out_loc"], R["lse_loc"], R["cum_col"], R["cum_recv"]
    ext, halo_src, halo, csum = R["ext"], R["halo_src"], R["halo"], R["csum"]
    st_send, st_recv, cpart = R["st_send"], R["st_recv"], R["cpart"]
    t2_o, t2_l, s_o, s_l = R["t2_o"], R["t2_l"], R["s_o"], R["s_l"]
    ret_send, ret_recv, lse_send, lse_recv = (
        R["ret_send"], R["ret_recv"], R["lse_send"], R["lse_recv"],
    )
    d_send, d_recv, x_send, x_recv, parts = (
        R[n] for n in ("d_send", "d_recv", "x_send", "x_recv", "parts")
    )
    ld = R["ld"]
    n_sp = len(ROUTES)
    z = lax.axis_index("sp")
    me = lax.axis_index("tp")
    chip, core = me // 2, me % 2
    chips = n_tp // 2
    rows, width = x_hbm.shape
    conv_w = wci_hbm.shape[0]
    attn_w = wq_hbm.shape[0]
    heads = n_sp
    hd = attn_w // heads
    d_all = wci_hbm.shape[1]
    partner = chip * 2 + 1 - core

    def remote(src, dst, s, r, dev):
        return pltpu.make_async_remote_copy(
            src_ref=src, dst_ref=dst, send_sem=s, recv_sem=r, device_id=dev, device_id_type=MESH
        )

    def settle(ref, sem):
        pltpu.make_async_copy(ref, ref, sem).wait()

    def same_core(dist):
        return lax.rem(chip + dist, chips) * 2 + core

    def other_core(dist):
        return lax.rem(chip + dist, chips) * 2 + 1 - core

    def piece_owner(rel):
        return same_core(rel // 2) if rel % 2 == 0 else other_core(rel // 2)

    def piece_source(rel):
        back = chips - rel // 2
        return same_core(back) if rel % 2 == 0 else other_core(back)

    barrier = pltpu.get_barrier_semaphore()
    for rel in range(1, n_tp):
        pl.semaphore_signal(
            barrier, inc=1, device_id={"tp": piece_owner(rel)}, device_id_type=MESH
        )
    for dist in range(1, n_sp):
        pl.semaphore_signal(
            barrier, inc=1, device_id={"sp": lax.rem(z + dist, n_sp)}, device_id_type=MESH
        )

    own_copy = pltpu.make_async_copy(x_hbm, xg.at[0], ld.at[0])
    own_copy.start()
    small = [
        pltpu.make_async_copy(R[n + "_hbm"], R[n], ld.at[5 + i])
        for i, n in enumerate(("gain", "ck", "lng", "cum"))
    ]
    for c in small:
        c.start()
    qkv_w = 3 * attn_w
    own_copy.wait()
    for h in range(heads):
        for i, w in enumerate((wk_hbm, wv_hbm)):
            pltpu.make_async_copy(
                w.at[pl.ds(h * hd, hd)], wbuf.at[pl.ds((2 * h + i) * hd, hd)], ld.at[1]
            ).start()
    pltpu.make_async_copy(wq_hbm, wbuf.at[pl.ds(2 * attn_w, attn_w)], ld.at[1]).start()
    pltpu.make_async_copy(wci_hbm, wbuf.at[pl.ds(qkv_w, conv_w)], ld.at[2]).start()
    pltpu.make_async_copy(wcg_hbm, wbuf.at[pl.ds(qkv_w + conv_w, conv_w)], ld.at[2]).start()
    wco_copy = pltpu.make_async_copy(R["wco_hbm"], wco, ld.at[3])
    wao_copy = pltpu.make_async_copy(R["wao_hbm"], wao, ld.at[4])
    wco_copy.start()
    wao_copy.start()

    pl.semaphore_wait(barrier, n_tp - 1 + n_sp - 1)

    rc = rows // AG_CHUNKS

    def ag_copy(rel, relay, c):
        r = pl.ds(c * rc, rc)
        src, to = (xg.at[rel - 1, r], partner) if relay else (xg.at[0, r], piece_owner(rel))
        return remote(src, xg.at[rel, r], R["ag_s"], R["ag_r"].at[rel - 2, c], {"tp": to})

    order = [AG_CHUNKS - 1] + list(range(AG_CHUNKS - 1))
    for c in order:
        for dist in range(1, chips):
            ag_copy(2 * dist, False, c).start()
    pair_copy = remote(xg.at[0], xg.at[1], R["ag_s"], R["ag_r1"], {"tp": partner})
    pair_copy.start()
    small[3].wait()
    for dist in range(1, n_sp):
        remote(
            cum_ref, cum_recv.at[z], R["cs"], R["cr"], {"sp": lax.rem(z + dist, n_sp)}
        ).start()
    cum_recv[z] = cum_ref[...]
    small[0].wait()

    def prepare(rel, c0, n):
        r = pl.ds(c0, n)
        owner = piece_source(rel)
        raw = xg[rel, r].astype(f32)
        g = gain_ref[pl.ds(pl.multiple_of(owner * width, width), width)].astype(f32).reshape(1, width)
        xs[rel, r] = (raw * g).astype(bf16)
        return jnp.sum(raw * raw, axis=1, keepdims=True)

    def wcols(rel, first, n):
        owner = piece_source(rel)
        return wbuf[pl.ds(first, n), pl.ds(pl.multiple_of(owner * width, width), width)]

    ss[...] = prepare(0, 0, rows)
    settle(wbuf.at[pl.ds(0, qkv_w)], ld.at[1])
    acc[:, :qkv_w] = lax.dot_general(xs[0], wcols(0, 0, qkv_w), NT, preferred_element_type=f32)
    settle(wbuf.at[pl.ds(qkv_w, 2 * conv_w)], ld.at[2])
    acc[:, qkv_w:] = lax.dot_general(
        xs[0], wcols(0, qkv_w, 2 * conv_w), NT, preferred_element_type=f32
    )
    pair_copy.wait_recv()
    ss[...] += prepare(1, 0, rows)
    acc[...] += lax.dot_general(
        xs[1], wcols(1, 0, qkv_w + 2 * conv_w), NT, preferred_element_type=f32
    )

    half = rc // 2
    spans = (pl.ds(0, rc), pl.ds(rc, half))

    def finish(group):
        r = pl.ds(group[0] * rc, len(group) * rc)
        total = acc[r, :qkv_w]
        sq = ss[r]
        for dist in range(1, chips):
            for c in group:
                ag_copy(2 * dist + 1, True, c).wait_recv()
            sq = sq + prepare(2 * dist + 1, group[0] * rc, len(group) * rc)
            total = total + lax.dot_general(
                xs[2 * dist + 1, r],
                wcols(2 * dist + 1, 0, qkv_w),
                NT,
                preferred_element_type=f32,
            )
        rms = lax.rsqrt(sq / d_all + 1e-06)
        ss[r] = rms
        total = total * rms
        for i, c in enumerate(group):
            push(c, total[i * rc : (i + 1) * rc])

    def push(c, total):
        for h in range(heads):
            zsend[h, c, :rc] = total[:, 2 * h * hd : 2 * (h + 1) * hd].astype(bf16)
            q_h = total[:, 2 * attn_w + h * hd : 2 * attn_w + (h + 1) * hd]
            zsend[h, c, rc:] = jnp.concatenate([q_h[:half], q_h[half:]], axis=1).astype(bf16)
        for src, routes in enumerate(ROUTES):

            @pl.when(z == src)
            def _():
                for h, part, to, kind in routes:
                    dst = zx.at[c, spans[part]] if kind == OTHER else zrecv.at[src, c, spans[part]]
                    remote(
                        zsend.at[h, c, spans[part]], dst, R["zs"], R["zr"].at[kind], {"sp": to}
                    ).start()

    rim = halo.shape[0]
    halo_copy = remote(halo_src, halo, R["hs"], R["hr"], {"sp": lax.rem(z + 1, n_sp)})

    def gated(r):
        pre = acc[r, qkv_w:]
        for rel in range(2, n_tp):
            pre = pre + lax.dot_general(
                xs[rel, r], wcols(rel, qkv_w, 2 * conv_w), NT, preferred_element_type=f32
            )
        pre = pre * ss[r]
        return (pre[:, :conv_w] * jax.nn.sigmoid(pre[:, conv_w:])).astype(bf16)

    def relay(c):
        for dist in range(1, chips):
            ag_copy(2 * dist, False, c).wait_recv()
            ag_copy(2 * dist + 1, True, c).start()

    def add_crossed(group):
        r = pl.ds(group[0] * rc, len(group) * rc)
        for dist in range(1, chips):
            ss[r] += prepare(2 * dist, group[0] * rc, len(group) * rc)
            acc[r, :qkv_w] += lax.dot_general(
                xs[2 * dist, r], wcols(2 * dist, 0, qkv_w), NT, preferred_element_type=f32
            )

    relay(3)
    add_crossed(ROW_GROUPS[0])
    finish(ROW_GROUPS[0])
    relay(0)
    add_crossed(ROW_GROUPS[1])
    halo_src[...] = gated(pl.ds(rows - rim, rim))

    @pl.when(z < n_sp - 1)
    def _():
        halo_copy.start()

    relay(1)
    finish(ROW_GROUPS[1])
    relay(2)
    add_crossed(ROW_GROUPS[2])
    finish(ROW_GROUPS[2])

    glu = gated(pl.ds(0, rows))
    ext[rim:, :] = glu.astype(f32)
    scale = hd ** (-0.5)
    low = lax.broadcasted_iota(jnp.int32, (rc, 2 * hd), 1) < hd
    wide_k = -(-rows // 128)
    allowed = lax.broadcasted_iota(jnp.int32, (rows, rows), 0) <= lax.broadcasted_iota(
        jnp.int32, (rows, rows), 1
    )

    def take_keys(tile, r0):
        kv = tile.astype(f32)
        k_s[pl.ds(r0, rc)] = kv[:, :hd].astype(bf16)
        v_s[pl.ds(r0, rc)] = jnp.where(low, pltpu.roll(kv, hd, 1), 1.0).astype(bf16)

    def take_queries(tile, r0):
        qt = tile.astype(f32) * scale
        q_s[pl.ds(r0, half)] = qt[:, :hd].astype(bf16)
        q_s[pl.ds(r0 + half, half)] = qt[:, hd:].astype(bf16)

    def attend(q, k, vt, cum_k, causal):
        sc = lax.dot_general(k, q, NT, preferred_element_type=f32) - cum_k
        if causal:
            sc = jnp.where(allowed, sc, -jnp.inf)
        top = jnp.max(sc, axis=0, keepdims=True)
        p = jnp.exp(sc - top).astype(bf16)
        both = jnp.dot(vt, p, preferred_element_type=f32)
        tot = both[hd : hd + 1]
        return both[:hd] / tot, top + jnp.log(tot)

    for h in range(heads):
        for c in range(AG_CHUNKS):
            take_keys(zsend[h, c, :rc], h * rows + c * rc)
            take_queries(zsend[h, c, rc:], h * rows + c * rc)
    v_t[...] = v_s[...].T
    for h in range(heads):
        own = pl.ds(h * rows, rows)
        own_cum = cum_ref[pl.ds(h, 1), :]
        col = jnp.broadcast_to(own_cum, (128, rows)).T
        out_loc[pl.ds(h * hd, hd), :], lse = attend(
            q_s[own], k_s[own], v_t[:, h * rows : (h + 1) * rows],
            jnp.concatenate([col] * wide_k, axis=1), True,
        )
        lse_loc[pl.ds(h, 1), :] = lse + own_cum

    qk_rows = half * 2 * hd * AG_CHUNKS // width

    taps = ck_ref.shape[0]
    blk = 64
    small[1].wait()
    small[2].wait()

    def conv_block(b, carry):
        first = pl.multiple_of(b * blk, blk)
        block = ext[pl.ds(first, blk + rim), :]
        tot = jnp.zeros((blk, conv_w), f32)
        for j in range(taps):
            off = rim - (taps - 1) + j
            tot = tot + block[off : off + blk] * ck_ref[j : j + 1, :].astype(f32)
        csum[pl.ds(first, blk), :] = tot
        return carry

    lax.fori_loop(1, rows // blk, conv_block, 0)

    @pl.when(z == 0)
    def _():
        halo[...] = jnp.zeros_like(halo)

    @pl.when(z > 0)
    def _():
        halo_copy.wait_recv()

    ext[:rim, :] = halo[...].astype(f32)
    conv_block(0, 0)
    cs = csum[...]
    first = jnp.sum(cs, axis=1, keepdims=True)
    second = jnp.sum(cs * cs, axis=1, keepdims=True)
    lane = lax.broadcasted_iota(jnp.int32, (rows, 128), 1)
    both = jnp.where(lane == 0, first, second)
    st_send[...] = both.T[: st_send.shape[0]]
    for rel in range(1, n_tp):
        remote(
            st_send, st_recv.at[rel - 1], R["st_s"], R["st_r"], {"tp": piece_owner(rel)}
        ).start()
    settle(cum_recv.at[pl.ds(0, n_sp - 1)], R["cr"])

    received = [[0] * 3 for _ in ROUTES]
    for routes in ROUTES:
        for _, part, to, kind in routes:
            received[to][kind] += 2 if part == KV else 1

    own_rows = rows // n_tp
    chip_rows = 2 * own_rows
    lanes = [
        pl.ds(pl.multiple_of(lax.rem(chip + 1 + i, chips) * chip_rows, chip_rows), chip_rows)
        for i in range(chips)
    ]

    def send_back(src_o, dst_o, src_l, dst_l, kind, to):
        remote(src_o, dst_o, R["rs"], R["rr"].at[kind], {"sp": to}).start()
        remote(src_l, dst_l, R["ls"], R["lr"].at[kind], {"sp": to}).start()

    def tile(zz, src, h, c):
        if src == zz:
            return zsend.at[h, c]
        return zrecv.at[src, c] if h == zz else zx.at[c]

    def far_terms(zz, h, r0, key_blks, query_blks):
        for i, b in enumerate(key_blks):
            for c in range(AG_CHUNKS):
                take_keys(tile(zz, b, h, c)[:rc], r0 + i * rows + c * rc)
            cum_col[pl.ds(r0 + i * rows, rows)] = jnp.broadcast_to(
                cum_recv[b, h : h + 1], (128, rows)
            ).T
        for i, b in enumerate(query_blks):
            for c in range(AG_CHUNKS):
                take_queries(tile(zz, b, h, c)[rc:], r0 + i * rows + c * rc)
        keys = slice(r0, r0 + len(key_blks) * rows)
        v_t[:, keys] = v_s[keys].T

    def far_attend(q, r0, n_k):
        keys = slice(r0, r0 + n_k)
        cum_k = jnp.concatenate([cum_col[keys]] * wide_k, axis=1)
        return attend(q, k_s[keys], v_t[:, keys], cum_k, False)

    def far_part(zz, tasks, seen):
        upper = zz // 2
        key_blk, query_blk = 2 * upper, 2 * upper + 1
        later = []

        def arrived(*kinds):
            for kind in kinds:
                if kind not in seen:
                    seen.add(kind)
                    n = received[zz][kind] * qk_rows
                    settle(xs.at[0, pl.ds(0, n)], R["zr"].at[kind])

        def hand_over(send, slot, i, to, o, lse):
            if to == zz:
                ret_recv[slot, i] = o.astype(bf16)
                lse_recv[slot, i] = lse
                return
            ret_send[send, i] = o.astype(bf16)
            lse_send[send, i] = lse
            args = (
                ret_send.at[send, i], ret_recv.at[slot, i],
                lse_send.at[send, i], lse_recv.at[slot, i], i, to,
            )
            if i == 0:
                send_back(*args)
            else:
                later.append(args)

        for kind, i in tasks:
            arrived(*((SAME, CROSS) if kind == CROSS else (kind,)))
            if kind == CROSS:
                if i == 0:
                    far_terms(zz, zz, 0, (0, 1), (2, 3))
                q = jnp.concatenate(
                    [
                        q_s[pl.ds(pl.multiple_of(b * rows + lanes[i].start, chip_rows), chip_rows)]
                        for b in range(2)
                    ],
                    axis=0,
                )
                o, lse = far_attend(q, 0, 2 * rows)
                for b in range(1, -1, -1):
                    o_b = o[:, b * chip_rows : (b + 1) * chip_rows]
                    lse_b = lse[:, b * chip_rows : (b + 1) * chip_rows]
                    lse_b = lse_b + cum_recv[2 + b, zz : zz + 1, lanes[i]]
                    if b == 1 and upper:
                        lse_n = s_l[:, lanes[i]]
                        top = jnp.maximum(lse_b, lse_n)
                        w_b, w_n = jnp.exp(lse_b - top), jnp.exp(lse_n - top)
                        tot = w_b + w_n
                        o_b = (o_b * w_b + s_o[:, lanes[i]] * w_n) / tot
                        lse_b = top + jnp.log(tot)
                    hand_over(b, zz, i, 2 + b, o_b, lse_b)
                continue
            h, r0 = (zz, 2 * rows) if kind == SAME else (OTHER_HEAD[zz], 3 * rows)
            far_terms(zz, h, r0, (key_blk,), (query_blk,))
            o, lse = far_attend(q_s[r0 : r0 + rows], r0, rows)
            o_ref, l_ref = (s_o, s_l) if kind == SAME else (t2_o, t2_l)
            o_ref[...] = o
            l_ref[...] = lse + cum_recv[query_blk, h : h + 1]
            if kind == OTHER or not upper:
                for n in range(chips):
                    hand_over(
                        kind + 1, h + 4 * upper if kind == OTHER else h, n, query_blk,
                        o_ref[:, lanes[n]], l_ref[:, lanes[n]],
                    )
        for args in later:
            send_back(*args)

    for zz in range(n_sp):

        @pl.when(z == zz)
        def _():
            far_part(zz, TASKS[zz], set())

    settle(st_recv, R["st_r"])
    tot = st_send[...]
    for rel in range(1, n_tp):
        tot = tot + st_recv[rel - 1]
    wide = jnp.concatenate([tot] * (128 // tot.shape[0]), axis=0).T
    mean = wide[:, 0:1] / CONV_CH
    var = wide[:, 1:2] / CONV_CH - mean * mean
    normed = (csum[...] - mean) * lax.rsqrt(var + 1e-05) * lng_ref[...].astype(f32).reshape(1, conv_w)
    conv_out = (normed / (1.0 + jnp.exp(-normed))).astype(bf16)
    wco_copy.wait()
    cpart[...] = jnp.dot(conv_out, wco[...], preferred_element_type=f32)

    def merge(h, slot, i):
        r = pl.ds(h * hd, hd)
        near, far = lse_loc[pl.ds(h, 1), lanes[i]], lse_recv[slot, i]
        top = jnp.maximum(near, far)
        w_near, w_far = jnp.exp(near - top), jnp.exp(far - top)
        tot = w_near + w_far
        out_loc[r, lanes[i]] = (
            out_loc[r, lanes[i]] * w_near + ret_recv[slot, i].astype(f32) * w_far
        ) / tot
        lse_loc[pl.ds(h, 1), lanes[i]] = top + jnp.log(tot)

    wao_copy.wait()
    cw = d_all // OUT_CHUNKS
    mine = pl.ds(pl.multiple_of(core * own_rows, own_rows), own_rows)
    theirs = pl.ds(pl.multiple_of((1 - core) * own_rows, own_rows), own_rows)

    def d_copy(dist, n):
        return remote(
            d_send.at[dist, n], d_recv.at[dist, n], R["ds"], R["dr"].at[dist, n], {"tp": partner}
        )

    def x_copy(n):
        return remote(x_send.at[n], x_recv.at[n], R["xs_s"], R["xr"].at[n], {"tp": same_core(1)})

    def exchange(dist):
        i = chips - 1 - dist

        for zz, n in ((1, 2), (2, 3), (3, 4)):

            @pl.when(z == zz)
            def _():
                settle(ret_recv.at[pl.ds(0, n), i], R["rr"].at[i])
                settle(lse_recv.at[pl.ds(0, n), i], R["lr"].at[i])
                for slot in range(6 if zz == 3 else heads):
                    merge(slot % heads, slot, i)

        att = out_loc[:, lanes[i]].T.astype(bf16)
        for n in range(OUT_CHUNKS):
            cols = slice(n * cw, (n + 1) * cw)
            parts[dist, n] = cpart[lanes[i], cols] + jnp.dot(
                att, wao[:, cols], preferred_element_type=f32
            )
            d_send[dist, n] = parts[dist, n, theirs].astype(bf16)
            d_copy(dist, n).start()

    exchange(1)
    for zz, tasks in enumerate(LATE_TASKS):
        if tasks:

            @pl.when(z == zz)
            def _():
                far_part(zz, tasks, {CROSS, SAME, OTHER})

    for n in range(OUT_CHUNKS):
        d_copy(1, n).wait_recv()
        x_send[n] = (parts[1, n, mine] + d_recv[1, n].astype(f32)).astype(bf16)
        x_copy(n).start()
    exchange(0)
    log_ref[...] = lse_loc[...]
    for n in range(OUT_CHUNKS):
        d_copy(0, n).wait_recv()
        tot = parts[0, n, mine] + d_recv[0, n].astype(f32)
        x_copy(n).wait_recv()
        tot = tot + x_recv[n].astype(f32)
        out_ref[:, n * cw : (n + 1) * cw] = tot.astype(bf16)

    settle(xg.at[pl.ds(1, n_tp - 1)], R["ag_s"])
    settle(cum_recv.at[pl.ds(0, n_sp - 1)], R["cs"])
    settle(st_recv, R["st_s"])
    settle(d_send, R["ds"])
    settle(x_send, R["xs_s"])

    @pl.when(z < n_sp - 1)
    def _():
        halo_copy.wait_send()

    sent = [sum(2 if r[1] == KV else 1 for r in routes) for routes in ROUTES]
    for src, (n, back) in enumerate(zip(sent, (4, 2, 2, 1), strict=True)):

        @pl.when(z == src)
        def _():
            settle(xs.at[0, pl.ds(0, n * qk_rows)], R["zs"])
            settle(ret_recv.at[pl.ds(0, back)], R["rs"])
            settle(lse_recv.at[pl.ds(0, back)], R["ls"])


def write_out(m_ref, l_ref, m_hbm, l_hbm, sem):
    a = pltpu.make_async_copy(m_ref, m_hbm, sem.at[0])
    b = pltpu.make_async_copy(l_ref, l_hbm, sem.at[1])
    a.start()
    b.start()
    a.wait()
    b.wait()


ARGS = (
    "x_hbm", "gain_hbm", "wci_hbm", "wcg_hbm", "ck_hbm", "lng_hbm",
    "wq_hbm", "wk_hbm", "wv_hbm", "cum_hbm", "wco_hbm", "wao_hbm",
)


def fused_local(n_tp, *args):
    f32, bf16 = jnp.float32, jnp.bfloat16
    inputs, norm_gain, w_conv_in, _, conv_kernel, ln_gain, w_query, _, _, cum_gate, _, _ = args
    n_sp = len(ROUTES)
    rows, width = inputs.shape
    conv_w, d_all = w_conv_in.shape
    attn_w = w_query.shape[0]
    heads = cum_gate.shape[0]
    hd = attn_w // heads
    chips = n_tp // 2
    own_rows = rows // n_tp
    rc = rows // AG_CHUNKS
    rim = -(-(conv_kernel.shape[0] - 1) // 16) * 16
    cw = d_all // OUT_CHUNKS
    all_w = 3 * attn_w + 2 * conv_w
    dma = pltpu.SemaphoreType.DMA
    vm = pltpu.VMEM
    scratch = {
        "xg": vm((n_tp, rows, width), bf16),
        "xs": vm((n_tp, rows, width), bf16),
        "wbuf": vm((all_w, d_all), bf16),
        "wco": vm((conv_w, d_all), bf16),
        "wao": vm((attn_w, d_all), bf16),
        "gain": vm(norm_gain.shape, bf16),
        "ck": vm(conv_kernel.shape, bf16),
        "lng": vm(ln_gain.shape, bf16),
        "cum": vm(cum_gate.shape, f32),
        "acc": vm((rows, all_w), f32),
        "ss": vm((rows, 1), f32),
        "zsend": vm((n_sp, AG_CHUNKS, rc + rc // 2, 2 * hd), bf16),
        "zrecv": vm((n_sp, AG_CHUNKS, rc + rc // 2, 2 * hd), bf16),
        "zx": vm((AG_CHUNKS, rc + rc // 2, 2 * hd), bf16),
        "q_s": vm((n_sp * rows, hd), bf16),
        "k_s": vm((n_sp * rows, hd), bf16),
        "v_s": vm((n_sp * rows, 2 * hd), bf16),
        "v_t": vm((2 * hd, n_sp * rows), bf16),
        "out_loc": vm((attn_w, rows), f32),
        "lse_loc": vm((heads, rows), f32),
        "cum_col": vm((4 * rows, 128), f32),
        "cum_recv": vm((n_sp, heads, rows), f32),
        "ext": vm((rows + rim, conv_w), f32),
        "halo_src": vm((rim, conv_w), bf16),
        "halo": vm((rim, conv_w), bf16),
        "csum": vm((rows, conv_w), f32),
        "st_send": vm((8, rows), f32),
        "st_recv": vm((n_tp - 1, 8, rows), f32),
        "cpart": vm((rows, d_all), f32),
        "t2_o": vm((hd, rows), f32),
        "t2_l": vm((1, rows), f32),
        "s_o": vm((hd, rows), f32),
        "s_l": vm((1, rows), f32),
        "ret_send": vm((4, chips, hd, 2 * own_rows), bf16),
        "ret_recv": vm((6, chips, hd, 2 * own_rows), bf16),
        "lse_send": vm((4, chips, 1, 2 * own_rows), f32),
        "lse_recv": vm((6, chips, 1, 2 * own_rows), f32),
        "d_send": vm((chips, OUT_CHUNKS, own_rows, cw), bf16),
        "d_recv": vm((chips, OUT_CHUNKS, own_rows, cw), bf16),
        "x_send": vm((OUT_CHUNKS, own_rows, cw), bf16),
        "x_recv": vm((OUT_CHUNKS, own_rows, cw), bf16),
        "parts": vm((chips, OUT_CHUNKS, 2 * own_rows, cw), f32),
        "ld": dma((9,)),
        "ag_s": dma,
        "ag_r1": dma,
        "ag_r": dma((n_tp - 2, AG_CHUNKS)),
        "zs": dma,
        "zr": dma((3,)),
        "cs": dma,
        "cr": dma,
        "hs": dma,
        "hr": dma,
        "st_s": dma,
        "st_r": dma,
        "rs": dma,
        "ls": dma,
        "rr": dma((chips,)),
        "lr": dma((chips,)),
        "ds": dma,
        "dr": dma((chips, OUT_CHUNKS)),
        "xs_s": dma,
        "xr": dma((OUT_CHUNKS,)),
    }
    far = pl.BlockSpec(memory_space=pl.ANY)
    near = pl.BlockSpec(memory_space=pltpu.VMEM)
    results = pl.pallas_call(
        functools.partial(fused_kernel, n_tp, ARGS + ("out_ref", "log_ref") + tuple(scratch)),
        out_shape=(
            pltpu.VMEM((own_rows, d_all), bf16),
            pltpu.VMEM((heads, rows), f32),
        ),
        in_specs=[far] * len(ARGS),
        out_specs=(near, near),
        scratch_shapes=list(scratch.values()),
        compiler_params=pltpu.CompilerParams(
            collective_id=0, has_side_effects=True, vmem_limit_bytes=60 * 1024 * 1024
        ),
    )(*args)
    return pl.pallas_call(
        write_out,
        out_shape=(
            jax.ShapeDtypeStruct((own_rows, d_all), bf16),
            jax.ShapeDtypeStruct((heads, rows), f32),
        ),
        in_specs=[near, near],
        out_specs=(far, far),
        scratch_shapes=[dma((2,))],
    )(*[pltpu.with_memory_space_constraint(r, pltpu.VMEM) for r in results])


def solution(mesh):
    in_specs = (
        P(("grp", "sp"), "tp"),
        P(),
        P("tp", None),
        P("tp", None),
        P(None, "tp"),
        P("tp"),
        P("tp", None),
        P("tp", None),
        P("tp", None),
        P("tp", ("grp", "sp")),
        P("tp", None),
        P("tp", None),
    )
    out_specs = (P(("grp", "sp", "tp"), None), P("tp", ("grp", "sp")))
    heads_here = HEADS // mesh.shape["tp"]
    fits = heads_here == mesh.shape["sp"] == len(ROUTES) and mesh.shape["tp"] == 4
    body = functools.partial(fused_local, mesh.shape["tp"]) if fits else local
    return jax.shard_map(body, mesh=mesh, in_specs=in_specs, out_specs=out_specs, check_vma=False)
```

```python
import functools
import jax
import jax.numpy as jnp
from jax import lax
from jax.experimental import pallas as pl
from jax.experimental.pallas import tpu as pltpu
from jax.sharding import PartitionSpec as P

D = 2048
CONV_CH = 1024
HEADS = 16


neg_large = -1e30


def passed_along(block, axis, distance):
    devices = range(lax.axis_size(axis))
    route = [(i - distance, i) for i in devices if i - distance in devices]
    return lax.ppermute(block, axis, route)


def block_terms(q_blk, q_cum, k_blk, v_blk, k_cum, q_first, k_first):
    score_scale = q_blk.shape[2] ** (-0.5)
    scores = (
        jnp.einsum("qhd,khd->hqk", q_blk, k_blk, preferred_element_type=jnp.float32) * score_scale
    )
    scores = scores + q_cum[:, :, None] - k_cum[:, None, :]
    q_pos = q_first + jnp.arange(q_blk.shape[0], dtype=jnp.int32)
    k_pos = k_first + jnp.arange(k_blk.shape[0], dtype=jnp.int32)
    allowed = k_pos[None, :] <= q_pos[:, None]
    scores = jnp.where(allowed[None], scores, -jnp.inf)
    block_top = jnp.max(scores, axis=-1)
    weights = jnp.exp(scores - block_top[..., None])
    block_total = jnp.sum(weights, axis=-1)
    block_out = jnp.einsum(
        "hqk,khd->hqd", weights.astype(jnp.bfloat16), v_blk, preferred_element_type=jnp.float32
    ).astype(jnp.bfloat16)
    return (block_top, block_total, block_out)


def merge_terms(state, terms):
    top_now, total_now, acc_now = state
    block_top, block_total, block_out = terms
    top_new = jnp.maximum(top_now, block_top)
    keep_old = jnp.exp(top_now - top_new)
    keep_new = jnp.exp(block_top - top_new)
    return (
        top_new,
        total_now * keep_old + block_total * keep_new,
        acc_now * keep_old[..., None] + block_out.astype(jnp.float32) * keep_new[..., None],
    )


def local(
    inputs,
    norm_gain,
    w_conv_in,
    w_conv_gate,
    conv_kernel,
    ln_gain,
    w_query,
    w_key,
    w_value,
    cum_gate,
    w_conv_out,
    w_attn_out,
):
    rows_here = inputs.shape[0]
    conv_width = w_conv_in.shape[0]
    attn_width = w_query.shape[0]
    heads_here = cum_gate.shape[0]
    head_dim = attn_width // heads_here
    taps_count = conv_kernel.shape[0]
    w_all = jnp.concatenate([w_conv_in, w_conv_gate, w_query, w_key, w_value], axis=0)
    gain_all = norm_gain.astype(jnp.float32)
    contract_dims = (((1,), (1,)), ((), ()))
    piece_f = lax.all_gather(inputs, "tp", axis=1, tiled=True).astype(jnp.float32)
    scaled_piece = (piece_f * gain_all[None, :]).astype(jnp.bfloat16)
    raw_proj = lax.dot_general(
        scaled_piece, w_all, contract_dims, preferred_element_type=jnp.float32
    )
    squares = jnp.sum(piece_f * piece_f, axis=1)
    rms = lax.rsqrt(squares / D + 1e-06)[:, None]
    proj = raw_proj * rms
    conv_in = proj[:, :conv_width]
    conv_gate = proj[:, conv_width : 2 * conv_width]
    query = proj[:, 2 * conv_width : 2 * conv_width + attn_width].astype(jnp.bfloat16)
    key_rows = proj[:, 2 * conv_width + attn_width : 2 * conv_width + 2 * attn_width].astype(
        jnp.bfloat16
    )
    value = proj[:, 2 * conv_width + 2 * attn_width :].astype(jnp.bfloat16)
    glu = (conv_in * jax.nn.sigmoid(conv_gate)).astype(jnp.bfloat16)
    rim_rows = passed_along(glu[rows_here - (taps_count - 1) :], "sp", 1)
    extended = jnp.concatenate([rim_rows, glu], axis=0)
    kernel = conv_kernel.astype(jnp.float32)
    conv_sum = jnp.zeros((rows_here, conv_width), jnp.float32)
    for tap_idx in range(taps_count):
        conv_sum = (
            conv_sum
            + extended[tap_idx : tap_idx + rows_here].astype(jnp.float32) * kernel[tap_idx][None, :]
        )
    chan_first, chan_second = lax.psum(
        (jnp.sum(conv_sum, axis=1), jnp.sum(conv_sum * conv_sum, axis=1)), "tp"
    )
    chan_mean = (chan_first / CONV_CH)[:, None]
    chan_var = (chan_second / CONV_CH)[:, None] - chan_mean * chan_mean
    normed = (
        (conv_sum - chan_mean) * lax.rsqrt(chan_var + 1e-05) * ln_gain.astype(jnp.float32)[None, :]
    )
    conv_out = jax.nn.silu(normed).astype(jnp.bfloat16)
    q_heads = query.reshape(rows_here, heads_here, head_dim)
    cum_all = lax.all_gather(cum_gate.T, "sp", axis=0, tiled=True)
    own_first = lax.axis_index("sp") * rows_here
    start_state = (
        jnp.full((heads_here, rows_here), neg_large, jnp.float32),
        jnp.zeros((heads_here, rows_here), jnp.float32),
        jnp.zeros((heads_here, rows_here, head_dim), jnp.float32),
    )
    state = start_state
    k_piece = lax.all_gather(key_rows, "sp", axis=0, tiled=True)
    v_piece = lax.all_gather(value, "sp", axis=0, tiled=True)
    block_count = k_piece.shape[0] // rows_here
    k_split = k_piece.reshape(block_count, rows_here, heads_here, head_dim)
    v_split = v_piece.reshape(block_count, rows_here, heads_here, head_dim)

    def visit(carry, item):
        k_blk, v_blk, block_idx = item
        k_first = block_idx * rows_here
        k_cum = lax.dynamic_slice_in_dim(cum_all, k_first, rows_here, 0).T

        def take_block(inner):
            return merge_terms(
                inner, block_terms(q_heads, cum_gate, k_blk, v_blk, k_cum, own_first, k_first)
            )

        def skip_block(inner):
            return inner

        return (lax.cond(k_first <= own_first, take_block, skip_block, carry), None)

    state, unused = lax.scan(
        visit, state, (k_split, v_split, jnp.arange(block_count, dtype=jnp.int32))
    )
    top_all, total_all, acc_all = state
    attn_out = (
        (acc_all / total_all[..., None])
        .transpose(1, 0, 2)
        .reshape(rows_here, attn_width)
        .astype(jnp.bfloat16)
    )
    log_total = top_all + jnp.log(total_all)
    mixed = lax.psum_scatter(
        (
            jnp.dot(conv_out, w_conv_out, preferred_element_type=jnp.float32)
            + jnp.dot(attn_out, w_attn_out, preferred_element_type=jnp.float32)
        ).astype(jnp.bfloat16),
        "tp",
        scatter_dimension=0,
        tiled=True,
    )
    return (mixed, log_total)


AG_CHUNKS = 4
OUT_CHUNKS = 4
MESH = pl.DeviceIdType.MESH
NT = (((1,), (1,)), ((), ()))
KV, Q = 0, 1
CROSS, SAME, OTHER = 0, 1, 2
ROUTES = (
    ((3, KV, 3, CROSS), (2, KV, 2, CROSS), (1, KV, 1, SAME), (3, KV, 1, OTHER)),
    ((3, KV, 3, CROSS), (2, KV, 2, CROSS), (0, KV, 0, CROSS), (0, Q, 0, SAME), (2, Q, 0, OTHER)),
    ((0, Q, 0, CROSS), (1, Q, 1, CROSS), (3, Q, 3, CROSS), (3, KV, 3, SAME), (0, KV, 3, OTHER)),
    ((0, Q, 0, CROSS), (1, Q, 1, CROSS), (2, Q, 2, SAME), (1, Q, 2, OTHER)),
)
GREETINGS = (((1,), 0, ()), ((2, 3), 3, (0, 2, 3)), ((1, 3), 2, ()), ((1, 2), 2, ()))
OTHER_HEAD = (2, 3, 1, 0)
NORM, FORWARD, ACROSS, BESIDE = 3, 4, 5, 6
TASKS = (
    ((ACROSS, 0), (NORM, 0), (ACROSS, 1), (CROSS, 0), (FORWARD, 0), (SAME, 0), (OTHER, 0),
     (ACROSS, 2), (ACROSS, 3)),
    ((ACROSS, 0), (CROSS, 0), (SAME, 0), (ACROSS, 1), (NORM, 0), (OTHER, 0), (ACROSS, 2),
     (FORWARD, 0), (CROSS, 1), (ACROSS, 3)),
    ((ACROSS, 0), (SAME, 0), (OTHER, 0), (ACROSS, 1), (NORM, 0), (CROSS, 0), (FORWARD, 0),
     (ACROSS, 2), (CROSS, 1), (ACROSS, 3)),
    ((ACROSS, 0), (NORM, 0), (ACROSS, 1), (CROSS, 0), (FORWARD, 0), (SAME, 0), (ACROSS, 2),
     (OTHER, 0), (CROSS, 1), (ACROSS, 3)),
)
LATE_TASKS = (((CROSS, 1),), (), (), ())
W_PIECES = 4
ROW_GROUPS = ((3,), (0,), (1, 2))


def fused_kernel(n_tp, names, *refs):
    f32, bf16 = jnp.float32, jnp.bfloat16
    R = dict(zip(names, refs, strict=True))
    x_hbm, wci_hbm, wcg_hbm = R["x_hbm"], R["wci_hbm"], R["wcg_hbm"]
    wq_hbm, wk_hbm, wv_hbm = R["wq_hbm"], R["wk_hbm"], R["wv_hbm"]
    out_ref, log_ref = R["out_ref"], R["log_ref"]
    xg, xs, wbuf, wco, wao, acc, ss = (
        R[n] for n in ("xg", "xs", "wbuf", "wco", "wao", "acc", "ss")
    )
    gain_ref, ck_ref, lng_ref, cum_ref = R["gain"], R["ck"], R["lng"], R["cum"]
    zsend, zrecv, zx = R["zsend"], R["zrecv"], R["zx"]
    q_s, k_s, v_s, v_t = R["q_s"], R["k_s"], R["v_s"], R["v_t"]
    out_loc, lse_loc, cum_col, cum_recv = R["out_loc"], R["lse_loc"], R["cum_col"], R["cum_recv"]
    ext, halo_src, halo, csum = R["ext"], R["halo_src"], R["halo"], R["csum"]
    st_send, st_recv, cpart = R["st_send"], R["st_recv"], R["cpart"]
    t2_o, t2_l, s_o, s_l = R["t2_o"], R["t2_l"], R["s_o"], R["s_l"]
    ret_send, ret_recv = R["ret_send"], R["ret_recv"]
    d_send, d_recv, x_send, x_recv, parts = (
        R[n] for n in ("d_send", "d_recv", "x_send", "x_recv", "parts")
    )
    wall, conv_s, att_s, att_all = R["wall"], R["conv_s"], R["att_s"], R["att_all"]
    ld = R["ld"]
    n_sp = len(ROUTES)
    z = lax.axis_index("sp")
    me = lax.axis_index("tp")
    chip, core = me // 2, me % 2
    chips = n_tp // 2
    rows, width = x_hbm.shape
    conv_w = wci_hbm.shape[0]
    attn_w = wq_hbm.shape[0]
    heads = n_sp
    hd = attn_w // heads
    d_all = wci_hbm.shape[1]
    partner = chip * 2 + 1 - core
    grp = lax.axis_index("grp")

    def remote(src, dst, s, r, dev):
        return pltpu.make_async_remote_copy(
            src_ref=src, dst_ref=dst, send_sem=s, recv_sem=r, device_id=dev, device_id_type=MESH
        )

    def settle(ref, sem):
        pltpu.make_async_copy(ref, ref, sem).wait()

    def same_core(dist):
        return lax.rem(chip + dist, chips) * 2 + core

    def other_core(dist):
        return lax.rem(chip + dist, chips) * 2 + 1 - core

    def piece_owner(rel):
        return same_core(rel // 2) if rel % 2 == 0 else other_core(rel // 2)

    def piece_source(rel):
        back = chips - rel // 2
        return same_core(back) if rel % 2 == 0 else other_core(back)

    barrier = pltpu.get_barrier_semaphore()
    for rel in range(1, n_tp):
        pl.semaphore_signal(
            barrier, inc=1, device_id={"tp": piece_owner(rel)}, device_id_type=MESH
        )
    for src, (greeted, _, _) in enumerate(GREETINGS):

        @pl.when(z == src)
        def _():
            for to in greeted:
                pl.semaphore_signal(barrier, inc=1, device_id={"sp": to}, device_id_type=MESH)

    pl.semaphore_signal(barrier, inc=1, device_id={"grp": 1 - grp}, device_id_type=MESH)
    own_copy = pltpu.make_async_copy(x_hbm, xg.at[0], ld.at[0])
    own_copy.start()
    small = [
        pltpu.make_async_copy(R[n + "_hbm"], R[n], ld.at[5 + i])
        for i, n in enumerate(("gain", "ck", "lng", "cum"))
    ]
    for c in small:
        c.start()
    qkv_w = 3 * attn_w
    own_copy.wait()
    for h in range(heads):
        for i, w in enumerate((wk_hbm, wv_hbm)):
            pltpu.make_async_copy(
                w.at[pl.ds(h * hd, hd)], wbuf.at[pl.ds((2 * h + i) * hd, hd)], ld.at[1]
            ).start()
    pltpu.make_async_copy(wq_hbm, wbuf.at[pl.ds(2 * attn_w, attn_w)], ld.at[1]).start()
    pltpu.make_async_copy(wci_hbm, wbuf.at[pl.ds(qkv_w, conv_w)], ld.at[2]).start()
    pltpu.make_async_copy(wcg_hbm, wbuf.at[pl.ds(qkv_w + conv_w, conv_w)], ld.at[2]).start()
    wco_copy = pltpu.make_async_copy(R["wco_hbm"], wco, ld.at[3])
    summed = wao.shape[1]
    wao_copy = pltpu.make_async_copy(R["wao_hbm"].at[:, pl.ds(0, summed)], wao, ld.at[4])
    wall_copy = pltpu.make_async_copy(
        R["wao_hbm"].at[:, pl.ds(summed, d_all - summed)], wall.at[0], ld.at[9]
    )
    wco_copy.start()
    wao_copy.start()
    wall_copy.start()

    for src, (_, count, told) in enumerate(GREETINGS):

        @pl.when(z == src)
        def _():
            pl.semaphore_wait(barrier, n_tp - 1 + count + 1)
            for to in told:
                pl.semaphore_signal(R["ready"], inc=1, device_id={"sp": to}, device_id_type=MESH)


    rc = rows // AG_CHUNKS

    def ag_copy(rel, relay, c):
        r = pl.ds(c * rc, rc)
        src, to = (xg.at[rel - 1, r], partner) if relay else (xg.at[0, r], piece_owner(rel))
        return remote(src, xg.at[rel, r], R["ag_s"], R["ag_r"].at[rel - 2, c], {"tp": to})

    order = [AG_CHUNKS - 1] + list(range(AG_CHUNKS - 1))
    for c in order:
        for dist in range(1, chips):
            ag_copy(2 * dist, False, c).start()
    pair_copy = remote(xg.at[0], xg.at[1], R["ag_s"], R["ag_r1"], {"tp": partner})
    pair_copy.start()
    small[0].wait()

    def prepare(rel, c0, n):
        r = pl.ds(c0, n)
        owner = piece_source(rel)
        raw = xg[rel, r].astype(f32)
        g = gain_ref[pl.ds(pl.multiple_of(owner * width, width), width)].astype(f32).reshape(1, width)
        xs[rel, r] = (raw * g).astype(bf16)
        return jnp.sum(raw * raw, axis=1, keepdims=True)

    def wcols(rel, first, n):
        owner = piece_source(rel)
        return wbuf[pl.ds(first, n), pl.ds(pl.multiple_of(owner * width, width), width)]

    ss[...] = prepare(0, 0, rows)
    settle(wbuf.at[pl.ds(0, qkv_w)], ld.at[1])
    acc[:, :qkv_w] = lax.dot_general(xs[0], wcols(0, 0, qkv_w), NT, preferred_element_type=f32)
    settle(wbuf.at[pl.ds(qkv_w, 2 * conv_w)], ld.at[2])
    acc[:, qkv_w:] = lax.dot_general(
        xs[0], wcols(0, qkv_w, 2 * conv_w), NT, preferred_element_type=f32
    )
    pair_copy.wait_recv()
    ss[...] += prepare(1, 0, rows)
    acc[...] += lax.dot_general(
        xs[1], wcols(1, 0, qkv_w + 2 * conv_w), NT, preferred_element_type=f32
    )

    half = rc // 2
    spans = (pl.ds(0, rc), pl.ds(rc, half))

    def finish(group):
        r = pl.ds(group[0] * rc, len(group) * rc)
        total = acc[r, :qkv_w]
        sq = ss[r]
        for dist in range(1, chips):
            for c in group:
                ag_copy(2 * dist + 1, True, c).wait_recv()
            sq = sq + prepare(2 * dist + 1, group[0] * rc, len(group) * rc)
            total = total + lax.dot_general(
                xs[2 * dist + 1, r],
                wcols(2 * dist + 1, 0, qkv_w),
                NT,
                preferred_element_type=f32,
            )
        rms = lax.rsqrt(sq / d_all + 1e-06)
        ss[r] = rms
        total = total * rms
        for i, c in enumerate(group):
            push(c, total[i * rc : (i + 1) * rc])

    def push(c, total):
        for h in range(heads):
            zsend[h, c, :rc] = total[:, 2 * h * hd : 2 * (h + 1) * hd].astype(bf16)
            q_h = total[:, 2 * attn_w + h * hd : 2 * attn_w + (h + 1) * hd]
            zsend[h, c, rc:] = jnp.concatenate([q_h[:half], q_h[half:]], axis=1).astype(bf16)
        for src, routes in enumerate(ROUTES):

            @pl.when(z == src)
            def _():
                for h, part, to, kind in routes:
                    dst = zx.at[c, spans[part]] if kind == OTHER else zrecv.at[src, c, spans[part]]
                    remote(
                        zsend.at[h, c, spans[part]], dst, R["zs"], R["zr"].at[kind], {"sp": to}
                    ).start()

    rim = halo.shape[0]
    halo_copy = remote(halo_src, halo, R["hs"], R["hr"], {"sp": lax.rem(z + 1, n_sp)})

    def gated(r):
        pre = acc[r, qkv_w:]
        for rel in range(2, n_tp):
            pre = pre + lax.dot_general(
                xs[rel, r], wcols(rel, qkv_w, 2 * conv_w), NT, preferred_element_type=f32
            )
        pre = pre * ss[r]
        return (pre[:, :conv_w] * jax.nn.sigmoid(pre[:, conv_w:])).astype(bf16)

    def relay(c):
        for dist in range(1, chips):
            ag_copy(2 * dist, False, c).wait_recv()
            ag_copy(2 * dist + 1, True, c).start()

    def add_crossed(group):
        r = pl.ds(group[0] * rc, len(group) * rc)
        for dist in range(1, chips):
            ss[r] += prepare(2 * dist, group[0] * rc, len(group) * rc)
            acc[r, :qkv_w] += lax.dot_general(
                xs[2 * dist, r], wcols(2 * dist, 0, qkv_w), NT, preferred_element_type=f32
            )

    w_rows = attn_w // 2 // W_PIECES

    def w_piece(of, p):
        return pl.ds(pl.multiple_of(of * (attn_w // 2) + p * w_rows, w_rows), w_rows)

    def w_across(p):
        r = w_piece(grp, p)
        return remote(
            wall.at[0, r], wall.at[2, r], R["ws"], R["wx_r"].at[p], {"tp": same_core(1)}
        )

    def w_beside(p, of):
        r = w_piece(of, p)
        return remote(
            wall.at[2, r], wall.at[2, r], R["ws"], R["wy_r"].at[p], {"grp": 1 - grp}
        )

    def w_pair(p, of):
        r = w_piece(of, p)
        return remote(wall.at[2, r], wall.at[3, r], R["ws"], R["wd_r"], {"tp": partner})

    relay(3)
    add_crossed(ROW_GROUPS[0])
    @pl.when(z != 1)
    def _():
        pl.semaphore_wait(R["ready"], 1)

    small[3].wait()
    for dist in range(1, n_sp):
        remote(
            cum_ref, cum_recv.at[z], R["cs"], R["cr"], {"sp": lax.rem(z + dist, n_sp)}
        ).start()
    cum_recv[z] = cum_ref[...]
    finish(ROW_GROUPS[0])
    relay(0)
    add_crossed(ROW_GROUPS[1])
    halo_src[...] = gated(pl.ds(rows - rim, rim))

    @pl.when(z < n_sp - 1)
    def _():
        halo_copy.start()

    relay(1)
    finish(ROW_GROUPS[1])
    relay(2)
    wall_copy.wait()
    for p in range(W_PIECES // 2):
        w_across(p).start()
    add_crossed(ROW_GROUPS[2])
    finish(ROW_GROUPS[2])
    remote(wall.at[0], wall.at[1], R["ws"], R["wp_r"], {"tp": partner}).start()

    glu = gated(pl.ds(0, rows))
    ext[rim:, :] = glu.astype(f32)
    taps = ck_ref.shape[0]
    blk = 64
    small[1].wait()
    small[2].wait()

    def conv_block(b, carry):
        first = pl.multiple_of(b * blk, blk)
        block = ext[pl.ds(first, blk + rim), :]
        tot = jnp.zeros((blk, conv_w), f32)
        for j in range(taps):
            off = rim - (taps - 1) + j
            tot = tot + block[off : off + blk] * ck_ref[j : j + 1, :].astype(f32)
        csum[pl.ds(first, blk), :] = tot
        return carry

    lax.fori_loop(1, rows // blk, conv_block, 0)

    @pl.when(z == 0)
    def _():
        halo[...] = jnp.zeros_like(halo)

    @pl.when(z > 0)
    def _():
        halo_copy.wait_recv()

    ext[:rim, :] = halo[...].astype(f32)
    conv_block(0, 0)
    cs = csum[...]
    first = jnp.sum(cs, axis=1, keepdims=True)
    second = jnp.sum(cs * cs, axis=1, keepdims=True)
    lane = lax.broadcasted_iota(jnp.int32, (rows, 128), 1)
    both = jnp.where(lane == 0, first, second)
    st_send[...] = both.T[: st_send.shape[0]]
    for rel in range(1, n_tp):
        remote(
            st_send, st_recv.at[rel - 1], R["st_s"], R["st_r"], {"tp": piece_owner(rel)}
        ).start()
    for p in range(W_PIECES // 2, W_PIECES):
        w_across(p).start()
    scale = hd ** (-0.5)
    low = lax.broadcasted_iota(jnp.int32, (rc, 2 * hd), 1) < hd
    wide_k = -(-rows // 128)
    allowed = lax.broadcasted_iota(jnp.int32, (rows, rows), 0) <= lax.broadcasted_iota(
        jnp.int32, (rows, rows), 1
    )

    def take_keys(tile, r0):
        kv = tile.astype(f32)
        k_s[pl.ds(r0, rc)] = kv[:, :hd].astype(bf16)
        v_s[pl.ds(r0, rc)] = jnp.where(low, pltpu.roll(kv, hd, 1), 1.0).astype(bf16)

    def take_queries(tile, r0):
        qt = tile.astype(f32) * scale
        q_s[pl.ds(r0, half)] = qt[:, :hd].astype(bf16)
        q_s[pl.ds(r0 + half, half)] = qt[:, hd:].astype(bf16)

    def attend(q, k, vt, cum_k, causal):
        sc = lax.dot_general(k, q, NT, preferred_element_type=f32) - cum_k
        if causal:
            sc = jnp.where(allowed, sc, -jnp.inf)
        top = jnp.max(sc, axis=0, keepdims=True)
        p = jnp.exp(sc - top).astype(bf16)
        both = jnp.dot(vt, p, preferred_element_type=f32)
        tot = both[hd : hd + 1]
        return both[:hd] / tot, top + jnp.log(tot)

    for h in range(heads):
        for c in range(AG_CHUNKS):
            take_keys(zsend[h, c, :rc], h * rows + c * rc)
            take_queries(zsend[h, c, rc:], h * rows + c * rc)
    v_t[...] = v_s[...].T
    for h in range(heads):
        own = pl.ds(h * rows, rows)
        own_cum = cum_ref[pl.ds(h, 1), :]
        col = jnp.broadcast_to(own_cum, (128, rows)).T
        out_loc[pl.ds(h * hd, hd), :], lse = attend(
            q_s[own], k_s[own], v_t[:, h * rows : (h + 1) * rows],
            jnp.concatenate([col] * wide_k, axis=1), True,
        )
        lse_loc[pl.ds(h, 1), :] = lse + own_cum

    qk_rows = half * 2 * hd * AG_CHUNKS // width

    settle(cum_recv.at[pl.ds(0, n_sp - 1)], R["cr"])

    received = [[0] * 3 for _ in ROUTES]
    for routes in ROUTES:
        for _, part, to, kind in routes:
            received[to][kind] += 2 if part == KV else 1

    own_rows = rows // n_tp
    chip_rows = 2 * own_rows
    lanes = [
        pl.ds(pl.multiple_of(lax.rem(chip + 1 + i, chips) * chip_rows, chip_rows), chip_rows)
        for i in range(chips)
    ]

    def send_back(send, slot, i, to):
        remote(
            ret_send.at[send, i], ret_recv.at[slot, i], R["rs"], R["rr"].at[i], {"sp": to}
        ).start()

    def fill(ref, o, lse):
        ref[:hd] = o.astype(bf16)
        high = lse.astype(bf16)
        rest = lse - high.astype(f32)
        mid = rest.astype(bf16)
        low = rest - mid.astype(f32)
        row = lax.broadcasted_iota(jnp.int32, (16, lse.shape[1]), 0)
        terms = jnp.where(row == 0, high.astype(f32), jnp.where(row == 1, mid.astype(f32), low))
        ref[hd:] = terms.astype(bf16)

    cw = d_all // OUT_CHUNKS
    early = range(summed // cw, OUT_CHUNKS)

    def owned(tp):
        return pl.ds(pl.multiple_of(tp * own_rows, own_rows), own_rows)

    def span(n):
        return slice(n * cw, (n + 1) * cw)

    def d_copy(dist, n):
        return remote(
            d_send.at[dist, n], d_recv.at[dist, n], R["ds"], R["dr"].at[dist, n], {"tp": partner}
        )

    def x_copy(n):
        return remote(x_send.at[n], x_recv.at[n], R["xs_s"], R["xr"].at[n], {"tp": same_core(1)})

    def conv_norm():
        settle(st_recv, R["st_r"])
        tot = st_send[...]
        for rel in range(1, n_tp):
            tot = tot + st_recv[rel - 1]
        wide = jnp.concatenate([tot] * (128 // tot.shape[0]), axis=0).T
        mean = wide[:, 0:1] / CONV_CH
        var = wide[:, 1:2] / CONV_CH - mean * mean
        normed = (
            (csum[...] - mean)
            * lax.rsqrt(var + 1e-05)
            * lng_ref[...].astype(f32).reshape(1, conv_w)
        )
        conv_s[...] = (normed / (1.0 + jnp.exp(-normed))).astype(bf16)
        wco_copy.wait()
        cpart[...] = jnp.dot(conv_s[...], wco[...], preferred_element_type=f32)
        for dist, to in ((1, other_core(1)), (0, partner)):
            for n in early:
                d_send[dist, n] = cpart[owned(to), span(n)].astype(bf16)
                d_copy(dist, n).start()

    def conv_forward():
        for n in early:
            d_copy(1, n).wait_recv()
            x_send[n] = (cpart[owned(same_core(1)), span(n)] + d_recv[1, n].astype(f32)).astype(bf16)
            x_copy(n).start()

    def pass_across(p):
        w_across(p).wait_recv()
        w_beside(p, grp).start()
        w_pair(p, grp).start()

    def pass_beside(p):
        w_beside(p, 1 - grp).wait_recv()
        w_pair(p, 1 - grp).start()

    def tile(zz, src, h, c):
        if src == zz:
            return zsend.at[h, c]
        return zrecv.at[src, c] if h == zz else zx.at[c]

    def far_terms(zz, h, r0, key_blks, query_blks):
        for i, b in enumerate(key_blks):
            for c in range(AG_CHUNKS):
                take_keys(tile(zz, b, h, c)[:rc], r0 + i * rows + c * rc)
            cum_col[pl.ds(r0 + i * rows, rows)] = jnp.broadcast_to(
                cum_recv[b, h : h + 1], (128, rows)
            ).T
        for i, b in enumerate(query_blks):
            for c in range(AG_CHUNKS):
                take_queries(tile(zz, b, h, c)[rc:], r0 + i * rows + c * rc)
        keys = slice(r0, r0 + len(key_blks) * rows)
        v_t[:, keys] = v_s[keys].T

    def far_attend(q, r0, n_k):
        keys = slice(r0, r0 + n_k)
        cum_k = jnp.concatenate([cum_col[keys]] * wide_k, axis=1)
        return attend(q, k_s[keys], v_t[:, keys], cum_k, False)

    def far_part(zz, tasks, seen):
        upper = zz // 2
        key_blk, query_blk = 2 * upper, 2 * upper + 1
        later = []

        def arrived(*kinds):
            for kind in kinds:
                if kind not in seen:
                    seen.add(kind)
                    n = received[zz][kind] * qk_rows
                    settle(xs.at[0, pl.ds(0, n)], R["zr"].at[kind])

        def hand_over(send, slot, i, to, o, lse):
            fill((ret_recv.at[slot, i] if to == zz else ret_send.at[send, i]), o, lse)
            if to == zz:
                return
            if i == 0:
                send_back(send, slot, i, to)
            else:
                later.append((send, slot, i, to))

        for kind, i in tasks:
            if kind >= NORM:
                (conv_norm, conv_forward, pass_across, pass_beside)[kind - NORM](
                    *([i] if kind >= ACROSS else [])
                )
                continue
            arrived(*((SAME, CROSS) if kind == CROSS and zz in (1, 2) else (kind,)))
            if kind == CROSS:
                if i == 0:
                    far_terms(zz, zz, 0, (0, 1), (2, 3))
                q = jnp.concatenate(
                    [
                        q_s[pl.ds(pl.multiple_of(b * rows + lanes[i].start, chip_rows), chip_rows)]
                        for b in range(2)
                    ],
                    axis=0,
                )
                o, lse = far_attend(q, 0, 2 * rows)
                for b in range(1, -1, -1):
                    o_b = o[:, b * chip_rows : (b + 1) * chip_rows]
                    lse_b = lse[:, b * chip_rows : (b + 1) * chip_rows]
                    lse_b = lse_b + cum_recv[2 + b, zz : zz + 1, lanes[i]]
                    if b == 1 and zz == 2:
                        lse_n = s_l[:, lanes[i]]
                        top = jnp.maximum(lse_b, lse_n)
                        w_b, w_n = jnp.exp(lse_b - top), jnp.exp(lse_n - top)
                        tot = w_b + w_n
                        o_b = (o_b * w_b + s_o[:, lanes[i]] * w_n) / tot
                        lse_b = top + jnp.log(tot)
                    hand_over(b, zz, i, 2 + b, o_b, lse_b)
                continue
            h, r0 = (zz, 2 * rows) if kind == SAME else (OTHER_HEAD[zz], 3 * rows)
            far_terms(zz, h, r0, (key_blk,), (query_blk,))
            o, lse = far_attend(q_s[r0 : r0 + rows], r0, rows)
            o_ref, l_ref = (s_o, s_l) if kind == SAME and zz == 2 else (t2_o, t2_l)
            o_ref[...] = o
            l_ref[...] = lse + cum_recv[query_blk, h : h + 1]
            if kind == OTHER or zz != 2:
                for n in range(chips):
                    hand_over(
                        kind + 1, 6 if kind == SAME and upper else h + 4 * upper * kind // OTHER,
                        n, query_blk,
                        o_ref[:, lanes[n]], l_ref[:, lanes[n]],
                    )
        for args in later:
            send_back(*args)

    for zz in range(n_sp):

        @pl.when(z == zz)
        def _():
            far_part(zz, TASKS[zz], set())

    def merge(h, slot, i):
        r = pl.ds(h * hd, hd)
        near, terms = lse_loc[pl.ds(h, 1), lanes[i]], ret_recv[slot, i, hd:].astype(f32)
        far = terms[0:1] + terms[1:2] + terms[2:3]
        top = jnp.maximum(near, far)
        w_near, w_far = jnp.exp(near - top), jnp.exp(far - top)
        tot = w_near + w_far
        out_loc[r, lanes[i]] = (
            out_loc[r, lanes[i]] * w_near + ret_recv[slot, i, :hd].astype(f32) * w_far
        ) / tot
        lse_loc[pl.ds(h, 1), lanes[i]] = top + jnp.log(tot)

    pass_beside(0)
    wao_copy.wait()
    late = range(summed // cw)
    mine = pl.ds(pl.multiple_of(core * own_rows, own_rows), own_rows)
    theirs = pl.ds(pl.multiple_of((1 - core) * own_rows, own_rows), own_rows)

    def hand_rows(i, r, rel, to):
        return remote(
            att_s.at[i, r], att_all.at[rel], R["at_s"], R["at_r"].at[rel // 2], {"tp": to}
        )

    def exchange(dist):
        i = chips - 1 - dist
        for zz, n in ((1, 2), (2, 3), (3, 4)):

            @pl.when(z == zz)
            def _():
                settle(ret_recv.at[pl.ds(0, n), i], R["rr"].at[i])
                for slot in range(7 if zz == 3 else heads):
                    merge(3 if slot == 6 else slot % heads, slot, i)

        att = out_loc[:, lanes[i]].T.astype(bf16)
        att_s[i] = att
        if dist:
            hand_rows(i, mine, 2, same_core(1)).start()
            hand_rows(i, theirs, 3, other_core(1)).start()
        else:
            hand_rows(i, theirs, 1, partner).start()
        for n in late:
            parts[dist, n] = cpart[lanes[i], span(n)] + jnp.dot(
                att, wao[:, span(n)], preferred_element_type=f32
            )
            d_send[dist, n] = parts[dist, n, theirs].astype(bf16)
            d_copy(dist, n).start()

    exchange(1)
    for zz, tasks in enumerate(LATE_TASKS):
        if tasks:

            @pl.when(z == zz)
            def _():
                far_part(zz, tasks, {CROSS, SAME, OTHER})

    for n in late:
        d_copy(1, n).wait_recv()
        x_send[n] = (parts[1, n, mine] + d_recv[1, n].astype(f32)).astype(bf16)
        x_copy(n).start()
    exchange(0)
    log_ref[...] = lse_loc[...]
    for p in range(1, W_PIECES):
        pass_beside(p)
    settle(wall.at[1], R["wp_r"])
    whole = jnp.dot(att_s[1, mine], wall[0], preferred_element_type=f32)
    settle(att_all.at[1], R["at_r"].at[0])
    whole = whole + jnp.dot(att_all[1], wall[1], preferred_element_type=f32)
    settle(att_all.at[pl.ds(2, 2)], R["at_r"].at[1])
    whole = whole + jnp.dot(att_all[2], wall[2], preferred_element_type=f32)
    settle(wall.at[3], R["wd_r"])
    whole = whole + jnp.dot(att_all[3], wall[3], preferred_element_type=f32)
    for n in early:
        d_copy(0, n).wait_recv()
        x_copy(n).wait_recv()
        tot = whole[:, n * cw - summed : (n + 1) * cw - summed] + cpart[owned(me), span(n)]
        tot = tot + d_recv[0, n].astype(f32) + x_recv[n].astype(f32)
        out_ref[:, span(n)] = tot.astype(bf16)
    for n in late:
        d_copy(0, n).wait_recv()
        tot = parts[0, n, mine] + d_recv[0, n].astype(f32)
        x_copy(n).wait_recv()
        tot = tot + x_recv[n].astype(f32)
        out_ref[:, span(n)] = tot.astype(bf16)

    settle(wall.at[pl.ds(0, 3)], R["ws"])
    settle(att_all.at[pl.ds(0, 3)], R["at_s"])
    settle(xg.at[pl.ds(1, n_tp - 1)], R["ag_s"])
    settle(cum_recv.at[pl.ds(0, n_sp - 1)], R["cs"])
    settle(st_recv, R["st_s"])
    settle(d_send, R["ds"])
    settle(x_send, R["xs_s"])

    @pl.when(z < n_sp - 1)
    def _():
        halo_copy.wait_send()

    sent = [sum(2 if r[1] == KV else 1 for r in routes) for routes in ROUTES]
    for src, (n, back) in enumerate(zip(sent, (4, 2, 2, 1), strict=True)):

        @pl.when(z == src)
        def _():
            settle(xs.at[0, pl.ds(0, n * qk_rows)], R["zs"])
            settle(ret_recv.at[pl.ds(0, back)], R["rs"])


def write_out(m_ref, l_ref, m_hbm, l_hbm, sem):
    a = pltpu.make_async_copy(m_ref, m_hbm, sem.at[0])
    b = pltpu.make_async_copy(l_ref, l_hbm, sem.at[1])
    a.start()
    b.start()
    a.wait()
    b.wait()


ARGS = (
    "x_hbm", "gain_hbm", "wci_hbm", "wcg_hbm", "ck_hbm", "lng_hbm",
    "wq_hbm", "wk_hbm", "wv_hbm", "cum_hbm", "wco_hbm", "wao_hbm",
)


def fused_local(n_tp, *args):
    f32, bf16 = jnp.float32, jnp.bfloat16
    inputs, norm_gain, w_conv_in, _, conv_kernel, ln_gain, w_query, _, _, cum_gate, _, _ = args
    n_sp = len(ROUTES)
    rows, width = inputs.shape
    conv_w, d_all = w_conv_in.shape
    attn_w = w_query.shape[0]
    heads = cum_gate.shape[0]
    hd = attn_w // heads
    chips = n_tp // 2
    own_rows = rows // n_tp
    rc = rows // AG_CHUNKS
    rim = -(-(conv_kernel.shape[0] - 1) // 16) * 16
    cw = d_all // OUT_CHUNKS
    all_w = 3 * attn_w + 2 * conv_w
    dma = pltpu.SemaphoreType.DMA
    vm = pltpu.VMEM
    scratch = {
        "xg": vm((n_tp, rows, width), bf16),
        "xs": vm((n_tp, rows, width), bf16),
        "wbuf": vm((all_w, d_all), bf16),
        "wco": vm((conv_w, d_all), bf16),
        "wao": vm((attn_w, d_all // 2), bf16),
        "wall": vm((n_tp, attn_w, d_all // 2), bf16),
        "conv_s": vm((rows, conv_w), bf16),
        "att_s": vm((chips, 2 * own_rows, attn_w), bf16),
        "att_all": vm((n_tp, own_rows, attn_w), bf16),
        "gain": vm(norm_gain.shape, bf16),
        "ck": vm(conv_kernel.shape, bf16),
        "lng": vm(ln_gain.shape, bf16),
        "cum": vm(cum_gate.shape, f32),
        "acc": vm((rows, all_w), f32),
        "ss": vm((rows, 1), f32),
        "zsend": vm((n_sp, AG_CHUNKS, rc + rc // 2, 2 * hd), bf16),
        "zrecv": vm((n_sp, AG_CHUNKS, rc + rc // 2, 2 * hd), bf16),
        "zx": vm((AG_CHUNKS, rc + rc // 2, 2 * hd), bf16),
        "q_s": vm((n_sp * rows, hd), bf16),
        "k_s": vm((n_sp * rows, hd), bf16),
        "v_s": vm((n_sp * rows, 2 * hd), bf16),
        "v_t": vm((2 * hd, n_sp * rows), bf16),
        "out_loc": vm((attn_w, rows), f32),
        "lse_loc": vm((heads, rows), f32),
        "cum_col": vm((4 * rows, 128), f32),
        "cum_recv": vm((n_sp, heads, rows), f32),
        "ext": vm((rows + rim, conv_w), f32),
        "halo_src": vm((rim, conv_w), bf16),
        "halo": vm((rim, conv_w), bf16),
        "csum": vm((rows, conv_w), f32),
        "st_send": vm((8, rows), f32),
        "st_recv": vm((n_tp - 1, 8, rows), f32),
        "cpart": vm((rows, d_all), f32),
        "t2_o": vm((hd, rows), f32),
        "t2_l": vm((1, rows), f32),
        "s_o": vm((hd, rows), f32),
        "s_l": vm((1, rows), f32),
        "ret_send": vm((4, chips, hd + 16, 2 * own_rows), bf16),
        "ret_recv": vm((7, chips, hd + 16, 2 * own_rows), bf16),
        "d_send": vm((chips, OUT_CHUNKS, own_rows, cw), bf16),
        "d_recv": vm((chips, OUT_CHUNKS, own_rows, cw), bf16),
        "x_send": vm((OUT_CHUNKS, own_rows, cw), bf16),
        "x_recv": vm((OUT_CHUNKS, own_rows, cw), bf16),
        "parts": vm((chips, OUT_CHUNKS // 2, 2 * own_rows, cw), f32),
        "ld": dma((10,)),
        "ws": dma,
        "wp_r": dma,
        "wd_r": dma,
        "wx_r": dma((W_PIECES,)),
        "wy_r": dma((W_PIECES,)),
        "at_s": dma,
        "at_r": dma((2,)),
        "ready": pltpu.SemaphoreType.REGULAR,
        "ag_s": dma,
        "ag_r1": dma,
        "ag_r": dma((n_tp - 2, AG_CHUNKS)),
        "zs": dma,
        "zr": dma((3,)),
        "cs": dma,
        "cr": dma,
        "hs": dma,
        "hr": dma,
        "st_s": dma,
        "st_r": dma,
        "rs": dma,
        "rr": dma((chips,)),
        "ds": dma,
        "dr": dma((chips, OUT_CHUNKS)),
        "xs_s": dma,
        "xr": dma((OUT_CHUNKS,)),
    }
    far = pl.BlockSpec(memory_space=pl.ANY)
    near = pl.BlockSpec(memory_space=pltpu.VMEM)
    results = pl.pallas_call(
        functools.partial(fused_kernel, n_tp, ARGS + ("out_ref", "log_ref") + tuple(scratch)),
        out_shape=(
            pltpu.VMEM((own_rows, d_all), bf16),
            pltpu.VMEM((heads, rows), f32),
        ),
        in_specs=[far] * len(ARGS),
        out_specs=(near, near),
        scratch_shapes=list(scratch.values()),
        compiler_params=pltpu.CompilerParams(
            collective_id=0, has_side_effects=True, vmem_limit_bytes=60 * 1024 * 1024
        ),
    )(*args)
    return pl.pallas_call(
        write_out,
        out_shape=(
            jax.ShapeDtypeStruct((own_rows, d_all), bf16),
            jax.ShapeDtypeStruct((heads, rows), f32),
        ),
        in_specs=[near, near],
        out_specs=(far, far),
        scratch_shapes=[dma((2,))],
    )(*[pltpu.with_memory_space_constraint(r, pltpu.VMEM) for r in results])


def solution(mesh):
    in_specs = (
        P(("grp", "sp"), "tp"),
        P(),
        P("tp", None),
        P("tp", None),
        P(None, "tp"),
        P("tp"),
        P("tp", None),
        P("tp", None),
        P("tp", None),
        P("tp", ("grp", "sp")),
        P("tp", None),
        P("tp", None),
    )
    out_specs = (P(("grp", "sp", "tp"), None), P("tp", ("grp", "sp")))
    heads_here = HEADS // mesh.shape["tp"]
    fits = heads_here == mesh.shape["sp"] == len(ROUTES) and mesh.shape["tp"] == 4
    fits = fits and mesh.shape["grp"] == 2
    body = functools.partial(fused_local, mesh.shape["tp"]) if fits else local
    return jax.shard_map(body, mesh=mesh, in_specs=in_specs, out_specs=out_specs, check_vma=False)
```

```python
import functools
import jax
import jax.numpy as jnp
from jax import lax
from jax.experimental import pallas as pl
from jax.experimental.pallas import tpu as pltpu
from jax.sharding import PartitionSpec as P

D = 2048
CONV_CH = 1024
HEADS = 16


neg_large = -1e30


def passed_along(block, axis, distance):
    devices = range(lax.axis_size(axis))
    route = [(i - distance, i) for i in devices if i - distance in devices]
    return lax.ppermute(block, axis, route)


def block_terms(q_blk, q_cum, k_blk, v_blk, k_cum, q_first, k_first):
    score_scale = q_blk.shape[2] ** (-0.5)
    scores = (
        jnp.einsum("qhd,khd->hqk", q_blk, k_blk, preferred_element_type=jnp.float32) * score_scale
    )
    scores = scores + q_cum[:, :, None] - k_cum[:, None, :]
    q_pos = q_first + jnp.arange(q_blk.shape[0], dtype=jnp.int32)
    k_pos = k_first + jnp.arange(k_blk.shape[0], dtype=jnp.int32)
    allowed = k_pos[None, :] <= q_pos[:, None]
    scores = jnp.where(allowed[None], scores, -jnp.inf)
    block_top = jnp.max(scores, axis=-1)
    weights = jnp.exp(scores - block_top[..., None])
    block_total = jnp.sum(weights, axis=-1)
    block_out = jnp.einsum(
        "hqk,khd->hqd", weights.astype(jnp.bfloat16), v_blk, preferred_element_type=jnp.float32
    ).astype(jnp.bfloat16)
    return (block_top, block_total, block_out)


def merge_terms(state, terms):
    top_now, total_now, acc_now = state
    block_top, block_total, block_out = terms
    top_new = jnp.maximum(top_now, block_top)
    keep_old = jnp.exp(top_now - top_new)
    keep_new = jnp.exp(block_top - top_new)
    return (
        top_new,
        total_now * keep_old + block_total * keep_new,
        acc_now * keep_old[..., None] + block_out.astype(jnp.float32) * keep_new[..., None],
    )


def local(
    inputs,
    norm_gain,
    w_conv_in,
    w_conv_gate,
    conv_kernel,
    ln_gain,
    w_query,
    w_key,
    w_value,
    cum_gate,
    w_conv_out,
    w_attn_out,
):
    rows_here = inputs.shape[0]
    conv_width = w_conv_in.shape[0]
    attn_width = w_query.shape[0]
    heads_here = cum_gate.shape[0]
    head_dim = attn_width // heads_here
    taps_count = conv_kernel.shape[0]
    w_all = jnp.concatenate([w_conv_in, w_conv_gate, w_query, w_key, w_value], axis=0)
    gain_all = norm_gain.astype(jnp.float32)
    contract_dims = (((1,), (1,)), ((), ()))
    piece_f = lax.all_gather(inputs, "tp", axis=1, tiled=True).astype(jnp.float32)
    scaled_piece = (piece_f * gain_all[None, :]).astype(jnp.bfloat16)
    raw_proj = lax.dot_general(
        scaled_piece, w_all, contract_dims, preferred_element_type=jnp.float32
    )
    squares = jnp.sum(piece_f * piece_f, axis=1)
    rms = lax.rsqrt(squares / D + 1e-06)[:, None]
    proj = raw_proj * rms
    conv_in = proj[:, :conv_width]
    conv_gate = proj[:, conv_width : 2 * conv_width]
    query = proj[:, 2 * conv_width : 2 * conv_width + attn_width].astype(jnp.bfloat16)
    key_rows = proj[:, 2 * conv_width + attn_width : 2 * conv_width + 2 * attn_width].astype(
        jnp.bfloat16
    )
    value = proj[:, 2 * conv_width + 2 * attn_width :].astype(jnp.bfloat16)
    glu = (conv_in * jax.nn.sigmoid(conv_gate)).astype(jnp.bfloat16)
    rim_rows = passed_along(glu[rows_here - (taps_count - 1) :], "sp", 1)
    extended = jnp.concatenate([rim_rows, glu], axis=0)
    kernel = conv_kernel.astype(jnp.float32)
    conv_sum = jnp.zeros((rows_here, conv_width), jnp.float32)
    for tap_idx in range(taps_count):
        conv_sum = (
            conv_sum
            + extended[tap_idx : tap_idx + rows_here].astype(jnp.float32) * kernel[tap_idx][None, :]
        )
    chan_first, chan_second = lax.psum(
        (jnp.sum(conv_sum, axis=1), jnp.sum(conv_sum * conv_sum, axis=1)), "tp"
    )
    chan_mean = (chan_first / CONV_CH)[:, None]
    chan_var = (chan_second / CONV_CH)[:, None] - chan_mean * chan_mean
    normed = (
        (conv_sum - chan_mean) * lax.rsqrt(chan_var + 1e-05) * ln_gain.astype(jnp.float32)[None, :]
    )
    conv_out = jax.nn.silu(normed).astype(jnp.bfloat16)
    q_heads = query.reshape(rows_here, heads_here, head_dim)
    cum_all = lax.all_gather(cum_gate.T, "sp", axis=0, tiled=True)
    own_first = lax.axis_index("sp") * rows_here
    start_state = (
        jnp.full((heads_here, rows_here), neg_large, jnp.float32),
        jnp.zeros((heads_here, rows_here), jnp.float32),
        jnp.zeros((heads_here, rows_here, head_dim), jnp.float32),
    )
    state = start_state
    k_piece = lax.all_gather(key_rows, "sp", axis=0, tiled=True)
    v_piece = lax.all_gather(value, "sp", axis=0, tiled=True)
    block_count = k_piece.shape[0] // rows_here
    k_split = k_piece.reshape(block_count, rows_here, heads_here, head_dim)
    v_split = v_piece.reshape(block_count, rows_here, heads_here, head_dim)

    def visit(carry, item):
        k_blk, v_blk, block_idx = item
        k_first = block_idx * rows_here
        k_cum = lax.dynamic_slice_in_dim(cum_all, k_first, rows_here, 0).T

        def take_block(inner):
            return merge_terms(
                inner, block_terms(q_heads, cum_gate, k_blk, v_blk, k_cum, own_first, k_first)
            )

        def skip_block(inner):
            return inner

        return (lax.cond(k_first <= own_first, take_block, skip_block, carry), None)

    state, unused = lax.scan(
        visit, state, (k_split, v_split, jnp.arange(block_count, dtype=jnp.int32))
    )
    top_all, total_all, acc_all = state
    attn_out = (
        (acc_all / total_all[..., None])
        .transpose(1, 0, 2)
        .reshape(rows_here, attn_width)
        .astype(jnp.bfloat16)
    )
    log_total = top_all + jnp.log(total_all)
    mixed = lax.psum_scatter(
        (
            jnp.dot(conv_out, w_conv_out, preferred_element_type=jnp.float32)
            + jnp.dot(attn_out, w_attn_out, preferred_element_type=jnp.float32)
        ).astype(jnp.bfloat16),
        "tp",
        scatter_dimension=0,
        tiled=True,
    )
    return (mixed, log_total)


AG_CHUNKS = 4
SUMMED_EIGHTHS = 3
MESH = pl.DeviceIdType.MESH
NT = (((1,), (1,)), ((), ()))
KV, Q = 0, 1
CROSS, SAME, OTHER = 0, 1, 2
ROUTES = (
    ((3, KV, 3, CROSS), (2, KV, 2, CROSS), (1, KV, 1, SAME), (3, KV, 1, OTHER)),
    ((3, KV, 3, CROSS), (2, KV, 2, CROSS), (0, KV, 0, CROSS), (0, Q, 0, SAME), (2, Q, 0, OTHER)),
    ((0, Q, 0, CROSS), (1, Q, 1, CROSS), (3, Q, 3, CROSS), (3, KV, 3, SAME), (0, KV, 3, OTHER)),
    ((0, Q, 0, CROSS), (1, Q, 1, CROSS), (2, Q, 2, SAME), (1, Q, 2, OTHER)),
)
GREETINGS = (((1,), 0, ()), ((2, 3), 3, (0, 2, 3)), ((1, 3), 2, ()), ((1, 2), 2, ()))
OTHER_HEAD = (2, 3, 1, 0)
NORM, FORWARD, SUMS, ACROSS, EXCHANGE = 3, 4, 5, 6, 7
TASKS = (
    ((ACROSS, 0), (NORM, 0), (EXCHANGE, 1), (ACROSS, 1), (CROSS, 0), (FORWARD, 0), (OTHER, 0),
     (SAME, 0), (SUMS, 0), (ACROSS, 2), (ACROSS, 3), (OTHER, 1), (SAME, 1), (CROSS, 1)),
    ((ACROSS, 0), (CROSS, 0), (NORM, 0), (ACROSS, 1), (SAME, 0), (FORWARD, 0), (OTHER, 0),
     (ACROSS, 2), (CROSS, 1), (ACROSS, 3)),
    ((ACROSS, 0), (SAME, 0), (OTHER, 0), (ACROSS, 1), (NORM, 0), (CROSS, 0), (FORWARD, 0),
     (ACROSS, 2), (CROSS, 1), (ACROSS, 3)),
    ((ACROSS, 0), (NORM, 0), (ACROSS, 1), (CROSS, 0), (FORWARD, 0), (SAME, 0), (ACROSS, 2),
     (OTHER, 0), (CROSS, 1), (ACROSS, 3)),
)
W_PIECES = 4
ROW_GROUPS = ((3,), (0,), (1, 2))


def fused_kernel(n_tp, names, *refs):
    f32, bf16 = jnp.float32, jnp.bfloat16
    R = dict(zip(names, refs, strict=True))
    x_hbm, wci_hbm, wcg_hbm = R["x_hbm"], R["wci_hbm"], R["wcg_hbm"]
    wq_hbm, wk_hbm, wv_hbm = R["wq_hbm"], R["wk_hbm"], R["wv_hbm"]
    out_ref, log_ref = R["out_ref"], R["log_ref"]
    xg, xs, wbuf, wco, wao, acc, ss = (
        R[n] for n in ("xg", "xs", "wbuf", "wco", "wao", "acc", "ss")
    )
    gain_ref, ck_ref, lng_ref, cum_ref = R["gain"], R["ck"], R["lng"], R["cum"]
    zsend, zrecv, zx = R["zsend"], R["zrecv"], R["zx"]
    q_s, k_s, v_s, v_t = R["q_s"], R["k_s"], R["v_s"], R["v_t"]
    out_loc, lse_loc, cum_col, cum_recv = R["out_loc"], R["lse_loc"], R["cum_col"], R["cum_recv"]
    ext, halo_src, halo, csum = R["ext"], R["halo_src"], R["halo"], R["csum"]
    st_send, st_recv, cpart = R["st_send"], R["st_recv"], R["cpart"]
    t2_o, t2_l, s_o, s_l = R["t2_o"], R["t2_l"], R["s_o"], R["s_l"]
    ret_send, ret_recv = R["ret_send"], R["ret_recv"]
    d_send, d_recv, x_send, x_recv = (
        [R[f"{name}{n}"] for n in range(4)] for name in ("d_send", "d_recv", "x_send", "x_recv")
    )
    parts = R["parts"]
    wall, stat_s, att_s, att_all = R["wall"], R["stat_s"], R["att_s"], R["att_all"]
    ld = R["ld"]
    n_sp = len(ROUTES)
    z = lax.axis_index("sp")
    me = lax.axis_index("tp")
    chip, core = me // 2, me % 2
    chips = n_tp // 2
    rows, width = x_hbm.shape
    conv_w = wci_hbm.shape[0]
    attn_w = wq_hbm.shape[0]
    heads = n_sp
    hd = attn_w // heads
    d_all = wci_hbm.shape[1]
    partner = chip * 2 + 1 - core
    grp = lax.axis_index("grp")

    def remote(src, dst, s, r, dev):
        return pltpu.make_async_remote_copy(
            src_ref=src, dst_ref=dst, send_sem=s, recv_sem=r, device_id=dev, device_id_type=MESH
        )

    def settle(ref, sem):
        pltpu.make_async_copy(ref, ref, sem).wait()

    def same_core(dist):
        return lax.rem(chip + dist, chips) * 2 + core

    def other_core(dist):
        return lax.rem(chip + dist, chips) * 2 + 1 - core

    def piece_owner(rel):
        return same_core(rel // 2) if rel % 2 == 0 else other_core(rel // 2)

    def piece_source(rel):
        back = chips - rel // 2
        return same_core(back) if rel % 2 == 0 else other_core(back)

    barrier = pltpu.get_barrier_semaphore()
    for rel in range(1, n_tp):
        pl.semaphore_signal(
            barrier, inc=1, device_id={"tp": piece_owner(rel)}, device_id_type=MESH
        )
    for src, (greeted, _, _) in enumerate(GREETINGS):

        @pl.when(z == src)
        def _():
            for to in greeted:
                pl.semaphore_signal(barrier, inc=1, device_id={"sp": to}, device_id_type=MESH)

    pl.semaphore_signal(barrier, inc=1, device_id={"grp": 1 - grp}, device_id_type=MESH)
    own_copy = pltpu.make_async_copy(x_hbm, xg.at[0], ld.at[0])
    own_copy.start()
    small = [
        pltpu.make_async_copy(R[n + "_hbm"], R[n], ld.at[5 + i])
        for i, n in enumerate(("gain", "ck", "lng", "cum"))
    ]
    for c in small:
        c.start()
    qkv_w = 3 * attn_w
    own_copy.wait()
    for h in range(heads):
        for i, w in enumerate((wk_hbm, wv_hbm)):
            pltpu.make_async_copy(
                w.at[pl.ds(h * hd, hd)], wbuf.at[pl.ds((2 * h + i) * hd, hd)], ld.at[1]
            ).start()
    pltpu.make_async_copy(wq_hbm, wbuf.at[pl.ds(2 * attn_w, attn_w)], ld.at[1]).start()
    pltpu.make_async_copy(wci_hbm, wbuf.at[pl.ds(qkv_w, conv_w)], ld.at[2]).start()
    pltpu.make_async_copy(wcg_hbm, wbuf.at[pl.ds(qkv_w + conv_w, conv_w)], ld.at[2]).start()
    wco_copy = pltpu.make_async_copy(R["wco_hbm"], wco, ld.at[3])
    summed = wao.shape[1]
    wao_copy = pltpu.make_async_copy(R["wao_hbm"].at[:, pl.ds(0, summed)], wao, ld.at[4])
    wall_copy = pltpu.make_async_copy(
        R["wao_hbm"].at[:, pl.ds(summed, d_all - summed)], wall.at[0], ld.at[9]
    )
    wco_copy.start()
    wao_copy.start()
    wall_copy.start()

    for src, (_, count, told) in enumerate(GREETINGS):

        @pl.when(z == src)
        def _():
            pl.semaphore_wait(barrier, n_tp - 1 + count + 1)
            for to in told:
                pl.semaphore_signal(R["ready"], inc=1, device_id={"sp": to}, device_id_type=MESH)


    rc = rows // AG_CHUNKS

    def ag_copy(rel, relay, c):
        r = pl.ds(c * rc, rc)
        src, to = (xg.at[rel - 1, r], partner) if relay else (xg.at[0, r], piece_owner(rel))
        return remote(src, xg.at[rel, r], R["ag_s"], R["ag_r"].at[rel - 2, c], {"tp": to})

    order = [AG_CHUNKS - 1] + list(range(AG_CHUNKS - 1))
    for c in order:
        for dist in range(1, chips):
            ag_copy(2 * dist, False, c).start()
    pair_copy = remote(xg.at[0], xg.at[1], R["ag_s"], R["ag_r1"], {"tp": partner})
    pair_copy.start()
    small[0].wait()

    def prepare(rel, c0, n):
        r = pl.ds(c0, n)
        owner = piece_source(rel)
        raw = xg[rel, r].astype(f32)
        g = gain_ref[pl.ds(pl.multiple_of(owner * width, width), width)].astype(f32).reshape(1, width)
        xs[rel, r] = (raw * g).astype(bf16)
        return jnp.sum(raw * raw, axis=1, keepdims=True)

    def wcols(rel, first, n):
        owner = piece_source(rel)
        return wbuf[pl.ds(first, n), pl.ds(pl.multiple_of(owner * width, width), width)]

    ss[...] = prepare(0, 0, rows)
    settle(wbuf.at[pl.ds(0, qkv_w)], ld.at[1])
    acc[:, :qkv_w] = lax.dot_general(xs[0], wcols(0, 0, qkv_w), NT, preferred_element_type=f32)
    settle(wbuf.at[pl.ds(qkv_w, 2 * conv_w)], ld.at[2])
    acc[:, qkv_w:] = lax.dot_general(
        xs[0], wcols(0, qkv_w, 2 * conv_w), NT, preferred_element_type=f32
    )
    pair_copy.wait_recv()
    ss[...] += prepare(1, 0, rows)
    acc[...] += lax.dot_general(
        xs[1], wcols(1, 0, qkv_w + 2 * conv_w), NT, preferred_element_type=f32
    )

    half = rc // 2
    spans = (pl.ds(0, rc), pl.ds(rc, half))

    def finish(group):
        r = pl.ds(group[0] * rc, len(group) * rc)
        total = acc[r, :qkv_w]
        sq = ss[r]
        for dist in range(1, chips):
            for c in group:
                ag_copy(2 * dist + 1, True, c).wait_recv()
            sq = sq + prepare(2 * dist + 1, group[0] * rc, len(group) * rc)
            total = total + lax.dot_general(
                xs[2 * dist + 1, r],
                wcols(2 * dist + 1, 0, qkv_w),
                NT,
                preferred_element_type=f32,
            )
        rms = lax.rsqrt(sq / d_all + 1e-06)
        ss[r] = rms
        total = total * rms
        for i, c in enumerate(group):
            push(c, total[i * rc : (i + 1) * rc])

    def push(c, total):
        for h in range(heads):
            zsend[h, c, :rc] = total[:, 2 * h * hd : 2 * (h + 1) * hd].astype(bf16)
            q_h = total[:, 2 * attn_w + h * hd : 2 * attn_w + (h + 1) * hd]
            zsend[h, c, rc:] = jnp.concatenate([q_h[:half], q_h[half:]], axis=1).astype(bf16)
        for src, routes in enumerate(ROUTES):

            @pl.when(z == src)
            def _():
                for h, part, to, kind in routes:
                    dst = zx.at[c, spans[part]] if kind == OTHER else zrecv.at[src, c, spans[part]]
                    remote(
                        zsend.at[h, c, spans[part]], dst, R["zs"], R["zr"].at[kind], {"sp": to}
                    ).start()

    rim = halo.shape[0]
    halo_copy = remote(halo_src, halo, R["hs"], R["hr"], {"sp": lax.rem(z + 1, n_sp)})

    def gated(r):
        pre = acc[r, qkv_w:]
        for rel in range(2, n_tp):
            pre = pre + lax.dot_general(
                xs[rel, r], wcols(rel, qkv_w, 2 * conv_w), NT, preferred_element_type=f32
            )
        pre = pre * ss[r]
        return (pre[:, :conv_w] * jax.nn.sigmoid(pre[:, conv_w:])).astype(bf16)

    def relay(c):
        for dist in range(1, chips):
            ag_copy(2 * dist, False, c).wait_recv()
            ag_copy(2 * dist + 1, True, c).start()

    def add_crossed(group):
        r = pl.ds(group[0] * rc, len(group) * rc)
        for dist in range(1, chips):
            ss[r] += prepare(2 * dist, group[0] * rc, len(group) * rc)
            acc[r, :qkv_w] += lax.dot_general(
                xs[2 * dist, r], wcols(2 * dist, 0, qkv_w), NT, preferred_element_type=f32
            )

    w_rows = attn_w // 2 // W_PIECES

    def w_piece(of, p):
        return pl.ds(pl.multiple_of(of * (attn_w // 2) + p * w_rows, w_rows), w_rows)

    def w_across(p):
        r = w_piece(grp, p)
        return remote(
            wall.at[0, r], wall.at[2, r], R["ws"], R["wx_r"].at[p], {"tp": same_core(1)}
        )

    def w_beside(p, of):
        r = w_piece(of, p)
        return remote(
            wall.at[2, r], wall.at[2, r], R["ws"], R["wy_r"].at[p], {"grp": 1 - grp}
        )

    def w_pair(p, of):
        r = w_piece(of, p)
        return remote(wall.at[2, r], wall.at[3, r], R["ws"], R["wd_r"], {"tp": partner})

    relay(3)
    add_crossed(ROW_GROUPS[0])
    @pl.when(z != 1)
    def _():
        pl.semaphore_wait(R["ready"], 1)

    small[3].wait()
    for dist in range(1, n_sp):
        remote(
            cum_ref, cum_recv.at[z], R["cs"], R["cr"], {"sp": lax.rem(z + dist, n_sp)}
        ).start()
    cum_recv[z] = cum_ref[...]
    finish(ROW_GROUPS[0])
    relay(0)
    add_crossed(ROW_GROUPS[1])
    halo_src[...] = gated(pl.ds(rows - rim, rim))

    @pl.when(z < n_sp - 1)
    def _():
        halo_copy.start()

    relay(1)
    finish(ROW_GROUPS[1])
    relay(2)
    wall_copy.wait()
    for p in range(W_PIECES // 2):
        w_across(p).start()
    add_crossed(ROW_GROUPS[2])
    finish(ROW_GROUPS[2])
    remote(wall.at[0], wall.at[1], R["ws"], R["wp_r"], {"tp": partner}).start()

    glu = gated(pl.ds(0, rows))
    ext[rim:, :] = glu.astype(f32)
    taps = ck_ref.shape[0]
    blk = 64
    small[1].wait()
    small[2].wait()

    def conv_block(b, carry):
        first = pl.multiple_of(b * blk, blk)
        block = ext[pl.ds(first, blk + rim), :]
        tot = jnp.zeros((blk, conv_w), f32)
        for j in range(taps):
            off = rim - (taps - 1) + j
            tot = tot + block[off : off + blk] * ck_ref[j : j + 1, :].astype(f32)
        csum[pl.ds(first, blk), :] = tot
        return carry

    lax.fori_loop(1, rows // blk, conv_block, 0)

    @pl.when(z == 0)
    def _():
        halo[...] = jnp.zeros_like(halo)

    @pl.when(z > 0)
    def _():
        halo_copy.wait_recv()

    ext[:rim, :] = halo[...].astype(f32)
    conv_block(0, 0)
    cs = csum[...]
    first = jnp.sum(cs, axis=1, keepdims=True)
    second = jnp.sum(cs * cs, axis=1, keepdims=True)
    lane = lax.broadcasted_iota(jnp.int32, (rows, 128), 1)
    both = jnp.where(lane == 0, first, second)
    st_send[...] = both.T[: st_send.shape[0]]
    for rel in range(1, n_tp):
        remote(
            st_send, st_recv.at[rel - 1], R["st_s"], R["st_r"], {"tp": piece_owner(rel)}
        ).start()
    for p in range(W_PIECES // 2, W_PIECES):
        w_across(p).start()
    scale = hd ** (-0.5)
    low = lax.broadcasted_iota(jnp.int32, (rc, 2 * hd), 1) < hd
    wide_k = -(-rows // 128)
    allowed = lax.broadcasted_iota(jnp.int32, (rows, rows), 0) <= lax.broadcasted_iota(
        jnp.int32, (rows, rows), 1
    )

    def take_keys(tile, r0):
        kv = tile.astype(f32)
        k_s[pl.ds(r0, rc)] = kv[:, :hd].astype(bf16)
        v_s[pl.ds(r0, rc)] = jnp.where(low, pltpu.roll(kv, hd, 1), 1.0).astype(bf16)

    def take_queries(tile, r0):
        qt = tile.astype(f32) * scale
        q_s[pl.ds(r0, half)] = qt[:, :hd].astype(bf16)
        q_s[pl.ds(r0 + half, half)] = qt[:, hd:].astype(bf16)

    def attend(q, k, vt, cum_k, causal):
        sc = lax.dot_general(k, q, NT, preferred_element_type=f32) - cum_k
        if causal:
            sc = jnp.where(allowed, sc, -jnp.inf)
        top = jnp.max(sc, axis=0, keepdims=True)
        p = jnp.exp(sc - top).astype(bf16)
        both = jnp.dot(vt, p, preferred_element_type=f32)
        tot = both[hd : hd + 1]
        return both[:hd] / tot, top + jnp.log(tot)

    for h in range(heads):
        for c in range(AG_CHUNKS):
            take_keys(zsend[h, c, :rc], h * rows + c * rc)
            take_queries(zsend[h, c, rc:], h * rows + c * rc)
    v_t[...] = v_s[...].T
    for h in range(heads):
        own = pl.ds(h * rows, rows)
        own_cum = cum_ref[pl.ds(h, 1), :]
        col = jnp.broadcast_to(own_cum, (128, rows)).T
        out_loc[pl.ds(h * hd, hd), :], lse = attend(
            q_s[own], k_s[own], v_t[:, h * rows : (h + 1) * rows],
            jnp.concatenate([col] * wide_k, axis=1), True,
        )
        lse_loc[pl.ds(h, 1), :] = lse + own_cum

    qk_rows = half * 2 * hd * AG_CHUNKS // width

    settle(cum_recv.at[pl.ds(0, n_sp - 1)], R["cr"])

    received = [[0] * 3 for _ in ROUTES]
    for routes in ROUTES:
        for _, part, to, kind in routes:
            received[to][kind] += 2 if part == KV else 1

    own_rows = rows // n_tp
    chip_rows = 2 * own_rows
    lanes = [
        pl.ds(pl.multiple_of(lax.rem(chip + 1 + i, chips) * chip_rows, chip_rows), chip_rows)
        for i in range(chips)
    ]

    def send_back(send, slot, i, to):
        remote(
            ret_send.at[send, i], ret_recv.at[slot, i], R["rs"], R["rr"].at[i], {"sp": to}
        ).start()

    def fill(ref, o, lse):
        ref[:hd] = o.astype(bf16)
        high = lse.astype(bf16)
        rest = lse - high.astype(f32)
        mid = rest.astype(bf16)
        low = rest - mid.astype(f32)
        row = lax.broadcasted_iota(jnp.int32, (16, lse.shape[1]), 0)
        terms = jnp.where(row == 0, high.astype(f32), jnp.where(row == 1, mid.astype(f32), low))
        ref[hd:] = terms.astype(bf16)

    late, early = range(2), range(2, 4)

    def owned(tp):
        return pl.ds(pl.multiple_of(tp * own_rows, own_rows), own_rows)

    def span(n, base=0):
        w = (d_all - summed) // 2 if n in early else summed // 2
        first = (summed if n in early else 0) + n % 2 * w - base
        return slice(first, first + w)

    def d_copy(dist, n):
        return remote(
            d_send[n].at[dist], d_recv[n].at[dist], R["ds"].at[n], R["dr"].at[dist, n],
            {"tp": partner},
        )

    def x_copy(n):
        return remote(x_send[n], x_recv[n], R["xs_s"].at[n], R["xr"].at[n], {"tp": same_core(1)})

    def conv_norm():
        settle(st_recv, R["st_r"])
        tot = st_send[...]
        for rel in range(1, n_tp):
            tot = tot + st_recv[rel - 1]
        stat_s[...] = jnp.concatenate([tot] * (128 // tot.shape[0]), axis=0).T
        gain = lng_ref[...].astype(f32).reshape(1, conv_w)
        wco_copy.wait()
        wao_copy.wait()
        for i, (dist, to) in enumerate(((1, other_core(1)), (0, partner))):
            mean = stat_s[lanes[i], 0:1] / CONV_CH
            var = stat_s[lanes[i], 1:2] / CONV_CH - mean * mean
            normed = (csum[lanes[i]] - mean) * lax.rsqrt(var + 1e-05) * gain
            conv_out = (normed / (1.0 + jnp.exp(-normed))).astype(bf16)
            cpart[lanes[i]] = jnp.dot(conv_out, wco[...], preferred_element_type=f32)
            for n in early:
                d_send[n][dist] = cpart[owned(to), span(n)].astype(bf16)
                d_copy(dist, n).start()

    def conv_forward():
        for n in early:
            d_copy(1, n).wait_recv()
            x_send[n][...] = (
                cpart[owned(same_core(1)), span(n)] + d_recv[n][1].astype(f32)
            ).astype(bf16)
            x_copy(n).start()

    def pass_across(p):
        w_across(p).wait_recv()
        w_beside(p, grp).start()
        w_pair(p, grp).start()

    def pass_beside(p):
        w_beside(p, 1 - grp).wait_recv()
        w_pair(p, 1 - grp).start()

    def tile(zz, src, h, c):
        if src == zz:
            return zsend.at[h, c]
        return zrecv.at[src, c] if h == zz else zx.at[c]

    def far_terms(zz, h, r0, key_blks, query_blks):
        for i, b in enumerate(key_blks):
            for c in range(AG_CHUNKS):
                take_keys(tile(zz, b, h, c)[:rc], r0 + i * rows + c * rc)
            cum_col[pl.ds(r0 + i * rows, rows)] = jnp.broadcast_to(
                cum_recv[b, h : h + 1], (128, rows)
            ).T
        for i, b in enumerate(query_blks):
            for c in range(AG_CHUNKS):
                take_queries(tile(zz, b, h, c)[rc:], r0 + i * rows + c * rc)
        keys = slice(r0, r0 + len(key_blks) * rows)
        v_t[:, keys] = v_s[keys].T

    def far_attend(q, r0, n_k):
        keys = slice(r0, r0 + n_k)
        cum_k = jnp.concatenate([cum_col[keys]] * (q.shape[0] // 128), axis=1)
        return attend(q, k_s[keys], v_t[:, keys], cum_k, False)

    def far_part(zz, tasks, seen):
        upper = zz // 2
        key_blk, query_blk = 2 * upper, 2 * upper + 1
        later = []

        def arrived(*kinds):
            for kind in kinds:
                if kind not in seen:
                    seen.add(kind)
                    n = received[zz][kind] * qk_rows
                    settle(xs.at[0, pl.ds(0, n)], R["zr"].at[kind])

        def hand_over(send, slot, i, to, o, lse):
            fill((ret_recv.at[slot, i] if to == zz else ret_send.at[send, i]), o, lse)
            if to == zz:
                return
            if i == 0:
                send_back(send, slot, i, to)
            else:
                later.append((send, slot, i, to))

        for kind, i in tasks:
            if kind >= NORM:
                (conv_norm, conv_forward, sum_forward, pass_across, exchange)[kind - NORM](
                    *([i] if kind >= ACROSS else [])
                )
                continue
            arrived(*((SAME, CROSS) if kind == CROSS and zz in (1, 2) else (kind,)))
            if kind == CROSS:
                if i == 0:
                    far_terms(zz, zz, 0, (0, 1), (2, 3))
                q = jnp.concatenate(
                    [
                        q_s[pl.ds(pl.multiple_of(b * rows + lanes[i].start, chip_rows), chip_rows)]
                        for b in range(2)
                    ],
                    axis=0,
                )
                o, lse = far_attend(q, 0, 2 * rows)
                for b in range(1, -1, -1):
                    o_b = o[:, b * chip_rows : (b + 1) * chip_rows]
                    lse_b = lse[:, b * chip_rows : (b + 1) * chip_rows]
                    lse_b = lse_b + cum_recv[2 + b, zz : zz + 1, lanes[i]]
                    if b == 1 and zz == 2:
                        lse_n = s_l[:, lanes[i]]
                        top = jnp.maximum(lse_b, lse_n)
                        w_b, w_n = jnp.exp(lse_b - top), jnp.exp(lse_n - top)
                        tot = w_b + w_n
                        o_b = (o_b * w_b + s_o[:, lanes[i]] * w_n) / tot
                        lse_b = top + jnp.log(tot)
                    hand_over(b, zz, i, 2 + b, o_b, lse_b)
                continue
            h, r0 = (zz, 2 * rows) if kind == SAME else (OTHER_HEAD[zz], 3 * rows)
            if i == 0:
                far_terms(zz, h, r0, (key_blk,), (query_blk,))
            if zz == 0:
                q = q_s[pl.ds(pl.multiple_of(r0 + lanes[i].start, chip_rows), chip_rows)]
                o, lse = far_attend(q, r0, rows)
                lse = lse + cum_recv[query_blk, h : h + 1, lanes[i]]
                hand_over(kind + 1, h, i, query_blk, o, lse)
                continue
            o, lse = far_attend(q_s[r0 : r0 + rows], r0, rows)
            o_ref, l_ref = (s_o, s_l) if kind == SAME and zz == 2 else (t2_o, t2_l)
            o_ref[...] = o
            l_ref[...] = lse + cum_recv[query_blk, h : h + 1]
            if kind == OTHER or zz != 2:
                for n in range(chips):
                    hand_over(
                        kind + 1, 6 if kind == SAME and upper else h + 4 * upper * kind // OTHER,
                        n, query_blk,
                        o_ref[:, lanes[n]], l_ref[:, lanes[n]],
                    )
        for args in later:
            send_back(*args)

    def merge(h, slot, i):
        r = pl.ds(h * hd, hd)
        near, terms = lse_loc[pl.ds(h, 1), lanes[i]], ret_recv[slot, i, hd:].astype(f32)
        far = terms[0:1] + terms[1:2] + terms[2:3]
        top = jnp.maximum(near, far)
        w_near, w_far = jnp.exp(near - top), jnp.exp(far - top)
        tot = w_near + w_far
        out_loc[r, lanes[i]] = (
            out_loc[r, lanes[i]] * w_near + ret_recv[slot, i, :hd].astype(f32) * w_far
        ) / tot
        lse_loc[pl.ds(h, 1), lanes[i]] = top + jnp.log(tot)

    mine = pl.ds(pl.multiple_of(core * own_rows, own_rows), own_rows)
    theirs = pl.ds(pl.multiple_of((1 - core) * own_rows, own_rows), own_rows)

    def hand_rows(i, r, rel, to):
        return remote(
            att_s.at[i, r], att_all.at[rel], R["at_s"], R["at_r"].at[rel // 2], {"tp": to}
        )

    def exchange(dist):
        i = chips - 1 - dist
        for zz, n in ((1, 2), (2, 3), (3, 4)):

            @pl.when(z == zz)
            def _():
                settle(ret_recv.at[pl.ds(0, n), i], R["rr"].at[i])
                for slot in range(7 if zz == 3 else heads):
                    merge(3 if slot == 6 else slot % heads, slot, i)

        att = out_loc[:, lanes[i]].T.astype(bf16)
        att_s[i] = att
        if dist:
            hand_rows(i, mine, 2, same_core(1)).start()
            hand_rows(i, theirs, 3, other_core(1)).start()
        else:
            hand_rows(i, theirs, 1, partner).start()
        for n in late:
            parts[dist, n] = cpart[lanes[i], span(n)] + jnp.dot(
                att, wao[:, span(n)], preferred_element_type=f32
            )
            d_send[n][dist] = parts[dist, n, theirs].astype(bf16)
            d_copy(dist, n).start()

    def sum_forward():
        for n in late:
            d_copy(1, n).wait_recv()
            x_send[n][...] = (parts[1, n, mine] + d_recv[n][1].astype(f32)).astype(bf16)
            x_copy(n).start()

    for zz in range(n_sp):

        @pl.when(z == zz)
        def _():
            far_part(zz, TASKS[zz], set())

    pass_beside(0)

    @pl.when(z > 0)
    def _():
        exchange(1)
        sum_forward()

    exchange(0)
    log_ref[...] = lse_loc[...]
    for p in range(1, W_PIECES):
        pass_beside(p)
    settle(wall.at[1], R["wp_r"])
    whole = jnp.dot(att_s[1, mine], wall[0], preferred_element_type=f32)
    settle(att_all.at[1], R["at_r"].at[0])
    whole = whole + jnp.dot(att_all[1], wall[1], preferred_element_type=f32)
    settle(att_all.at[pl.ds(2, 2)], R["at_r"].at[1])
    whole = whole + jnp.dot(att_all[2], wall[2], preferred_element_type=f32)
    settle(wall.at[3], R["wd_r"])
    whole = whole + jnp.dot(att_all[3], wall[3], preferred_element_type=f32)
    for n in early:
        d_copy(0, n).wait_recv()
        x_copy(n).wait_recv()
        tot = whole[:, span(n, summed)] + cpart[owned(me), span(n)]
        tot = tot + d_recv[n][0].astype(f32) + x_recv[n][...].astype(f32)
        out_ref[:, span(n)] = tot.astype(bf16)
    for n in late:
        d_copy(0, n).wait_recv()
        tot = parts[0, n, mine] + d_recv[n][0].astype(f32)
        x_copy(n).wait_recv()
        tot = tot + x_recv[n][...].astype(f32)
        out_ref[:, span(n)] = tot.astype(bf16)

    settle(wall.at[pl.ds(0, 3)], R["ws"])
    settle(att_all.at[pl.ds(0, 3)], R["at_s"])
    settle(xg.at[pl.ds(1, n_tp - 1)], R["ag_s"])
    settle(cum_recv.at[pl.ds(0, n_sp - 1)], R["cs"])
    settle(st_recv, R["st_s"])
    for n in range(4):
        settle(d_send[n], R["ds"].at[n])
        settle(x_send[n], R["xs_s"].at[n])

    @pl.when(z < n_sp - 1)
    def _():
        halo_copy.wait_send()

    sent = [sum(2 if r[1] == KV else 1 for r in routes) for routes in ROUTES]
    for src, (n, back) in enumerate(zip(sent, (4, 2, 2, 1), strict=True)):

        @pl.when(z == src)
        def _():
            settle(xs.at[0, pl.ds(0, n * qk_rows)], R["zs"])
            settle(ret_recv.at[pl.ds(0, back)], R["rs"])


def write_out(m_ref, l_ref, m_hbm, l_hbm, sem):
    a = pltpu.make_async_copy(m_ref, m_hbm, sem.at[0])
    b = pltpu.make_async_copy(l_ref, l_hbm, sem.at[1])
    a.start()
    b.start()
    a.wait()
    b.wait()


ARGS = (
    "x_hbm", "gain_hbm", "wci_hbm", "wcg_hbm", "ck_hbm", "lng_hbm",
    "wq_hbm", "wk_hbm", "wv_hbm", "cum_hbm", "wco_hbm", "wao_hbm",
)


def fused_local(n_tp, *args):
    f32, bf16 = jnp.float32, jnp.bfloat16
    inputs, norm_gain, w_conv_in, _, conv_kernel, ln_gain, w_query, _, _, cum_gate, _, _ = args
    n_sp = len(ROUTES)
    rows, width = inputs.shape
    conv_w, d_all = w_conv_in.shape
    attn_w = w_query.shape[0]
    heads = cum_gate.shape[0]
    hd = attn_w // heads
    chips = n_tp // 2
    own_rows = rows // n_tp
    rc = rows // AG_CHUNKS
    rim = -(-(conv_kernel.shape[0] - 1) // 16) * 16
    summed = d_all * SUMMED_EIGHTHS // 8
    widths = [summed // 2] * 2 + [(d_all - summed) // 2] * 2
    all_w = 3 * attn_w + 2 * conv_w
    dma = pltpu.SemaphoreType.DMA
    vm = pltpu.VMEM
    scratch = {
        "xg": vm((n_tp, rows, width), bf16),
        "xs": vm((n_tp, rows, width), bf16),
        "wbuf": vm((all_w, d_all), bf16),
        "wco": vm((conv_w, d_all), bf16),
        "wao": vm((attn_w, summed), bf16),
        "wall": vm((n_tp, attn_w, d_all - summed), bf16),
        "stat_s": vm((rows, 128), f32),
        "att_s": vm((chips, 2 * own_rows, attn_w), bf16),
        "att_all": vm((n_tp, own_rows, attn_w), bf16),
        "gain": vm(norm_gain.shape, bf16),
        "ck": vm(conv_kernel.shape, bf16),
        "lng": vm(ln_gain.shape, bf16),
        "cum": vm(cum_gate.shape, f32),
        "acc": vm((rows, all_w), f32),
        "ss": vm((rows, 1), f32),
        "zsend": vm((n_sp, AG_CHUNKS, rc + rc // 2, 2 * hd), bf16),
        "zrecv": vm((n_sp, AG_CHUNKS, rc + rc // 2, 2 * hd), bf16),
        "zx": vm((AG_CHUNKS, rc + rc // 2, 2 * hd), bf16),
        "q_s": vm((n_sp * rows, hd), bf16),
        "k_s": vm((n_sp * rows, hd), bf16),
        "v_s": vm((n_sp * rows, 2 * hd), bf16),
        "v_t": vm((2 * hd, n_sp * rows), bf16),
        "out_loc": vm((attn_w, rows), f32),
        "lse_loc": vm((heads, rows), f32),
        "cum_col": vm((4 * rows, 128), f32),
        "cum_recv": vm((n_sp, heads, rows), f32),
        "ext": vm((rows + rim, conv_w), f32),
        "halo_src": vm((rim, conv_w), bf16),
        "halo": vm((rim, conv_w), bf16),
        "csum": vm((rows, conv_w), f32),
        "st_send": vm((8, rows), f32),
        "st_recv": vm((n_tp - 1, 8, rows), f32),
        "cpart": vm((rows, d_all), f32),
        "t2_o": vm((hd, rows), f32),
        "t2_l": vm((1, rows), f32),
        "s_o": vm((hd, rows), f32),
        "s_l": vm((1, rows), f32),
        "ret_send": vm((4, chips, hd + 16, 2 * own_rows), bf16),
        "ret_recv": vm((7, chips, hd + 16, 2 * own_rows), bf16),
        **{f"d_send{n}": vm((chips, own_rows, w), bf16) for n, w in enumerate(widths)},
        **{f"d_recv{n}": vm((chips, own_rows, w), bf16) for n, w in enumerate(widths)},
        **{f"x_send{n}": vm((own_rows, w), bf16) for n, w in enumerate(widths)},
        **{f"x_recv{n}": vm((own_rows, w), bf16) for n, w in enumerate(widths)},
        "parts": vm((chips, 2, 2 * own_rows, summed // 2), f32),
        "ld": dma((10,)),
        "ws": dma,
        "wp_r": dma,
        "wd_r": dma,
        "wx_r": dma((W_PIECES,)),
        "wy_r": dma((W_PIECES,)),
        "at_s": dma,
        "at_r": dma((2,)),
        "ready": pltpu.SemaphoreType.REGULAR,
        "ag_s": dma,
        "ag_r1": dma,
        "ag_r": dma((n_tp - 2, AG_CHUNKS)),
        "zs": dma,
        "zr": dma((3,)),
        "cs": dma,
        "cr": dma,
        "hs": dma,
        "hr": dma,
        "st_s": dma,
        "st_r": dma,
        "rs": dma,
        "rr": dma((chips,)),
        "ds": dma((4,)),
        "dr": dma((chips, 4)),
        "xs_s": dma((4,)),
        "xr": dma((4,)),
    }
    far = pl.BlockSpec(memory_space=pl.ANY)
    near = pl.BlockSpec(memory_space=pltpu.VMEM)
    results = pl.pallas_call(
        functools.partial(fused_kernel, n_tp, ARGS + ("out_ref", "log_ref") + tuple(scratch)),
        out_shape=(
            pltpu.VMEM((own_rows, d_all), bf16),
            pltpu.VMEM((heads, rows), f32),
        ),
        in_specs=[far] * len(ARGS),
        out_specs=(near, near),
        scratch_shapes=list(scratch.values()),
        compiler_params=pltpu.CompilerParams(
            collective_id=0, has_side_effects=True, vmem_limit_bytes=60 * 1024 * 1024
        ),
    )(*args)
    return pl.pallas_call(
        write_out,
        out_shape=(
            jax.ShapeDtypeStruct((own_rows, d_all), bf16),
            jax.ShapeDtypeStruct((heads, rows), f32),
        ),
        in_specs=[near, near],
        out_specs=(far, far),
        scratch_shapes=[dma((2,))],
    )(*[pltpu.with_memory_space_constraint(r, pltpu.VMEM) for r in results])


def solution(mesh):
    in_specs = (
        P(("grp", "sp"), "tp"),
        P(),
        P("tp", None),
        P("tp", None),
        P(None, "tp"),
        P("tp"),
        P("tp", None),
        P("tp", None),
        P("tp", None),
        P("tp", ("grp", "sp")),
        P("tp", None),
        P("tp", None),
    )
    out_specs = (P(("grp", "sp", "tp"), None), P("tp", ("grp", "sp")))
    heads_here = HEADS // mesh.shape["tp"]
    fits = heads_here == mesh.shape["sp"] == len(ROUTES) and mesh.shape["tp"] == 4
    fits = fits and mesh.shape["grp"] == 2
    body = functools.partial(fused_local, mesh.shape["tp"]) if fits else local
    return jax.shard_map(body, mesh=mesh, in_specs=in_specs, out_specs=out_specs, check_vma=False)
```
